256 devices in a mesh: ep: 16 (over y, x), tp: 16 (over z, core).
Axes of the slice: x: 4, y: 4, z: 8, core: 2. Of those that a mesh axis runs over, the one named last changes fastest.
Arguments:
- query_rows: bfloat16 [16384, 2048], P('ep', 'tp'), may hold values from -6 to 6
- key_rows: bfloat16 [16384, 2048], P('ep', 'tp'), may hold values from -6 to 6
- value_rows: bfloat16 [16384, 4096], P('ep', 'tp'), may hold values from -6 to 6
- gate_rows: bfloat16 [16384, 4096], P('ep', 'tp'), may hold values from -6 to 6
- log_decay: float32 [16, 16384], P('tp', 'ep'), may hold values from -1.5 to 0
- out_weight: bfloat16 [4096, 2048], P('tp'), may hold values from -0.09375 to 0.09375
- channel_input: bfloat16 [12288, 2048], P(('ep', 'tp')), may hold values from -6 to 6
- norm_gain: float32 [2048], replicated, may hold values from 0.1 to 1.9
- routes: int32 [12288, 2], P(('ep', 'tp')), may hold values from 0 to 31, all different within a row; in each aligned block of 48 rows (0 to 47, 48 to 95, ...) at most 5 rows name the same one
- route_weight: float32 [12288, 2], P(('ep', 'tp')), may hold values from 0.2 to 1.5
- expert_gate: bfloat16 [32, 2048, 2048], P('ep', None, 'tp'), may hold values from -0.125 to 0.125
- expert_up: bfloat16 [32, 2048, 2048], P('ep', None, 'tp'), may hold values from -0.125 to 0.125
- expert_down: bfloat16 [32, 2048, 2048], P('ep', 'tp'), may hold values from -0.125 to 0.125
- shared_gate: bfloat16 [2048, 2048], P(None, 'tp'), may hold values from -0.125 to 0.125
- shared_up: bfloat16 [2048, 2048], P(None, 'tp'), may hold values from -0.125 to 0.125
- shared_down: bfloat16 [2048, 2048], P('tp'), may hold values from -0.125 to 0.125
Outputs:
- mixer_out: bfloat16 [16384, 2048], P(('ep', 'tp'))
- channel_out: bfloat16 [12288, 2048], P(('ep', 'tp'))
The draws below stay inside these ranges and needn't reach their ends.
Inputs may be any that keep to these rules, and one draw needn't show every extreme that they name: `routes`: each row names 2 different experts; among the rows of one device no expert is named more than 5 times, a bound that some block reaches.
All inputs are finite; a program needn't handle non-finite values.
Results may differ from the reference program's by a relative error of at most 0.02.
Values may be sent and summed in bfloat16 or wider, within the bound.
A program may use at most 128 MiB of HBM per device.

```python
import math
import jax
import jax.numpy as jnp
import numpy as np
from jax import lax

D = 2048
RETENTION_HEADS = 16
DK = 128
DV = 256
BLOCK = 128
TOK_A = 1024
FF = 2048
TOPK = 2
T_M = 48
SEQUENCE_LENGTH = 16384
QK_WIDTH = 2048
V_WIDTH = 4096
EXPERTS = 32
TOKENS_M = 12288
CAP = 5
N_EP = 16
N_TP = 16


def draw_log_decay(key, part):
    key_pieces_list = jax.random.split(jax.random.fold_in(key, 11), 7)
    slow_share = 0.5
    slow_heads = jax.random.uniform(key_pieces_list[0], (RETENTION_HEADS,)) < slow_share
    whole_loss = jax.random.uniform(key_pieces_list[1], (RETENTION_HEADS,), minval=0.1, maxval=0.5)
    fast_rate = jax.random.uniform(key_pieces_list[2], (RETENTION_HEADS,), minval=1.0 / 100.0, maxval=1.0 / 30.0)
    decay_rate = jnp.where(slow_heads, whole_loss / SEQUENCE_LENGTH, fast_rate)
    span_count = SEQUENCE_LENGTH // TOK_A
    block_factor = jnp.exp(jax.random.uniform(key_pieces_list[3], (RETENTION_HEADS, span_count), minval=-0.7, maxval=0.7))
    block_factor = jnp.repeat(block_factor, TOK_A, axis=1)
    jitter = jax.random.uniform(key_pieces_list[4], (RETENTION_HEADS, SEQUENCE_LENGTH), minval=0.5, maxval=1.5)
    steady_level = -(decay_rate[:, None] * block_factor * jitter)
    surge_position = jax.random.randint(key_pieces_list[5], (RETENTION_HEADS, 2), 0, SEQUENCE_LENGTH)
    surge_extent = jnp.log(jax.random.uniform(key_pieces_list[6], (RETENTION_HEADS, 2), minval=0.5, maxval=0.8))
    head_number = jnp.broadcast_to(jnp.arange(RETENTION_HEADS)[:, None], (RETENTION_HEADS, 2))
    surge_list = jnp.zeros((RETENTION_HEADS, SEQUENCE_LENGTH), jnp.float32).at[head_number, surge_position].add(surge_extent)
    return (steady_level + surge_list).astype(jnp.float32)


def block_scale(own_key, shape, cuts, least, largest):
    loudness = 1.0
    for dim, shards_of in cuts:
        steps = jax.random.uniform(jax.random.fold_in(jax.random.fold_in(own_key, 6), dim), (shards_of,), jnp.float32, least / len(cuts), largest / len(cuts))
        loudness = loudness * jnp.repeat(jnp.exp(steps), shape[dim] // shards_of).reshape((-1,) + (1,) * (len(shape) - 1 - dim))
    return loudness


def shared_out(rng, own, number, rows, number_of, top, most, slope):
    sequence = jax.random.permutation(rng, number_of)
    crowded, usual = shares(number_of, rows * top, most, slope, True), shares(number_of, rows * top, most, slope, False)
    places = jnp.arange(number_of)

    def named(tallies, rotation):
        used = int((tallies > 0).sum())
        fixed = max(1, used // 4)
        passed = fixed + (places - fixed + rotation * (used - fixed)) % max(1, number_of - fixed)
        return jnp.zeros((number_of,), jnp.int32).at[sequence[jnp.where(places < fixed, places, passed)]].set(jnp.asarray(tallies, jnp.int32))

    tallies = jnp.where(number % 4 == 0, named(crowded, number // 4), named(usual, number - number // 4 - 1))
    mixed = jax.random.permutation(jax.random.fold_in(own, 3), number_of)
    giver, sink = mixed[0:number_of // 2 * 2:2], mixed[1:number_of // 2 * 2:2]
    slack = jnp.minimum(tallies[giver] - 1, most - tallies[sink]) // 2
    slack = jnp.where((giver == sequence[0]) | (sink == sequence[0]) | (tallies[sink] == 0), 0, jnp.maximum(slack, 0))
    passed = jax.random.randint(jax.random.fold_in(own, 4), (number_of // 2,), 0, 1 << 20) % (slack + 1)
    tallies = tallies.at[giver].add(-passed).at[sink].add(passed)
    members = jnp.searchsorted(jnp.cumsum(tallies), jnp.arange(rows * top), side="right").astype(jnp.int32)
    listing = members.reshape(top, rows).T
    listing = listing[jax.random.permutation(jax.random.fold_in(own, 1), rows)]
    rotation = jax.random.randint(jax.random.fold_in(own, 2), (rows, 1), 0, top)
    return jnp.take_along_axis(listing, (jnp.arange(top)[None, :] + rotation) % top, axis=1)


def shares(amount, total, most, slope, full):
    loads = [(1 << 20) // math.isqrt(standing ** slope) + 1 for standing in range(1, amount + 1)]
    largest = most if full else min(most, max(-(-total // amount), total * loads[0] // sum(loads)))
    least = 1 if total - largest >= amount - 1 else 0
    given, spare = [largest] + [least] * (amount - 1), total - largest - least * (amount - 1)
    while spare > 0:
        free = [i for i in range(1, amount) if given[i] < largest] or [i for i in range(1, amount) if given[i] < most]
        whole, left = sum([loads[i] for i in free]), spare
        for i in free:
            addition = min(most - given[i], max(1, left * loads[i] // whole), spare)
            given[i] = given[i] + addition
            spare = spare - addition
    return np.array(given)


def noise(key, shape, scale, most, pieces=(), kind=jnp.bfloat16):
    values = scale * jax.random.normal(key, shape, jnp.float32)
    if pieces:
        values = values * block_scale(key, shape, pieces, -0.22, 0.18)
    return jnp.clip(values, -most, most).astype(kind)


def setup_inputs(seed: int = 0) -> dict:
    arg_keys = jax.random.split(jax.random.key(seed), 17)
    query_rows = noise(arg_keys[0], (SEQUENCE_LENGTH, QK_WIDTH), 1.0, 6.0, ((0, 16), (1, 16)))
    key_rows = noise(arg_keys[1], (SEQUENCE_LENGTH, QK_WIDTH), 1.0, 6.0, ((0, 16), (1, 16)))
    value_rows = noise(arg_keys[2], (SEQUENCE_LENGTH, V_WIDTH), 1.0, 6.0, ((0, 16), (1, 16)))
    gate_rows = noise(arg_keys[3], (SEQUENCE_LENGTH, V_WIDTH), 1.0, 6.0, ((0, 16), (1, 16)))
    log_decay = draw_log_decay(jax.random.fold_in(arg_keys[16], 71), 0)
    out_weight = noise(arg_keys[5], (V_WIDTH, D), V_WIDTH ** -0.5, 0.09375, ((0, 16),))
    channel_input = noise(arg_keys[6], (TOKENS_M, D), 1.0, 6.0, ((0, 256),))
    norm_gain = jnp.clip(1.0 + 0.18 * jax.random.normal(arg_keys[7], (D,), jnp.float32), 0.1, 1.9)
    routes_keys = jax.random.split(jax.random.fold_in(arg_keys[8], 1), TOKENS_M // T_M)
    routes_turns = jax.random.permutation(jax.random.fold_in(arg_keys[8], 3), TOKENS_M // T_M)
    routes = jax.vmap(lambda own, number: shared_out(jax.random.fold_in(arg_keys[8], 2), own, number, T_M, EXPERTS, TOPK, CAP, 1))(routes_keys, routes_turns).reshape((TOKENS_M, TOPK))
    route_weight = jnp.clip(0.2 + 1.3 * jax.random.uniform(arg_keys[9], (TOKENS_M, TOPK), jnp.float32) ** block_scale(arg_keys[9], (TOKENS_M, TOPK), ((0, 256),), -0.2, 0.2), 0.2, 1.5)
    expert_gate = noise(arg_keys[10], (EXPERTS, D, FF), D ** -0.5, 0.125, ((0, 16), (2, 16)))
    expert_up = noise(arg_keys[11], (EXPERTS, D, FF), D ** -0.5, 0.125, ((0, 16), (2, 16)))
    expert_down = noise(arg_keys[12], (EXPERTS, FF, D), FF ** -0.5, 0.125, ((0, 16), (1, 16)))
    shared_gate = noise(arg_keys[13], (D, FF), D ** -0.5, 0.125, ((1, 16),))
    shared_up = noise(arg_keys[14], (D, FF), D ** -0.5, 0.125, ((1, 16),))
    shared_down = noise(arg_keys[15], (FF, D), FF ** -0.5, 0.125, ((0, 16),))
    return {"query_rows": query_rows, "key_rows": key_rows, "value_rows": value_rows, "gate_rows": gate_rows, "log_decay": log_decay, "out_weight": out_weight, "channel_input": channel_input, "norm_gain": norm_gain, "routes": routes, "route_weight": route_weight, "expert_gate": expert_gate, "expert_up": expert_up, "expert_down": expert_down, "shared_gate": shared_gate, "shared_up": shared_up, "shared_down": shared_down}


epsilon = 1e-06
turn_base = 10000.0

def turn_heads(rows, position):
    half_width = rows.shape[-1] // 2
    inverse = turn_base ** (-jnp.arange(half_width, dtype=jnp.float32) / half_width)
    angles = position[:, None] * inverse[None, :]
    cosine = jnp.cos(angles)[:, None, :]
    sine = jnp.sin(angles)[:, None, :]
    widened = rows.astype(jnp.float32)
    first_half = widened[..., :half_width]
    second_half = widened[..., half_width:]
    turned = jnp.concatenate([first_half * cosine - second_half * sine, second_half * cosine + first_half * sine], axis=-1)
    return turned.astype(jnp.bfloat16)

def blocked_product(left, right, parts):
    width = right.shape[0] // parts

    def add_block(index, total):
        columns = lax.dynamic_slice_in_dim(left, index * width, width, 1)
        block_rows = lax.dynamic_slice_in_dim(right, index * width, width, 0)
        partial_sum = jnp.dot(columns, block_rows, preferred_element_type=jnp.float32).astype(jnp.bfloat16)
        partial_sum = lax.optimization_barrier(partial_sum)
        return total + partial_sum.astype(jnp.float32)
    return lax.fori_loop(0, parts, add_block, jnp.zeros((left.shape[0], right.shape[1]), jnp.float32))

def swiglu_hidden(rows, gate_weight, up_weight):
    gate_part = jnp.dot(rows, gate_weight, preferred_element_type=jnp.float32)
    up_part = jnp.dot(rows, up_weight, preferred_element_type=jnp.float32)
    return (jax.nn.silu(gate_part) * up_part).astype(jnp.bfloat16)

def retention(queries, keys_turned, values, log_decay):
    block_count = SEQUENCE_LENGTH // BLOCK
    query_blocks = queries.reshape(block_count, BLOCK, RETENTION_HEADS, DK)
    key_blocks = keys_turned.reshape(block_count, BLOCK, RETENTION_HEADS, DK)
    value_blocks = values.reshape(block_count, BLOCK, RETENTION_HEADS, DV)
    decay_blocks = jnp.transpose(log_decay.reshape(RETENTION_HEADS, block_count, BLOCK), (1, 0, 2))
    lower = jnp.arange(BLOCK)[:, None] >= jnp.arange(BLOCK)[None, :]
    highest = lax.Precision.HIGHEST

    def advance(state, inputs):
        query_block, key_block, value_block, decay_block = inputs
        running = jnp.cumsum(decay_block, axis=1)
        query_wide = query_block.astype(jnp.float32)
        key_wide = key_block.astype(jnp.float32)
        value_wide = value_block.astype(jnp.float32)
        scores = jnp.einsum('ihk,jhk->hij', query_wide, key_wide, precision=highest)
        spread = running[:, :, None] - running[:, None, :]
        weights = jnp.where(lower, scores * jnp.exp(jnp.where(lower, spread, 0.0)), 0.0).astype(jnp.bfloat16)
        intra = jnp.einsum('hij,jhe->ihe', weights.astype(jnp.float32), value_wide, precision=highest)
        query_decayed = query_wide * jnp.exp(running).T[:, :, None]
        inter = jnp.einsum('ihk,hke->ihe', query_decayed, state, precision=highest)
        block_end = running[:, -1]
        key_decayed = key_wide * jnp.exp(block_end[:, None] - running).T[:, :, None]
        update = jnp.einsum('jhk,jhe->hke', key_decayed, value_wide, precision=highest)
        new_state = jnp.exp(block_end)[:, None, None] * state + update
        return (new_state, intra + inter)
    start_state = jnp.zeros((RETENTION_HEADS, DK, DV), jnp.float32)
    _, outputs = lax.scan(advance, start_state, (query_blocks, key_blocks, value_blocks, decay_blocks))
    return outputs.reshape(SEQUENCE_LENGTH, RETENTION_HEADS, DV)

def reference(query_rows, key_rows, value_rows, gate_rows, log_decay, out_weight, channel_input, norm_gain, routes, route_weight, expert_gate, expert_up, expert_down, shared_gate, shared_up, shared_down):
    position = jnp.arange(SEQUENCE_LENGTH, dtype=jnp.int32).astype(jnp.float32)
    queries = turn_heads(query_rows.reshape(SEQUENCE_LENGTH, RETENTION_HEADS, DK), position)
    keys_turned = turn_heads(key_rows.reshape(SEQUENCE_LENGTH, RETENTION_HEADS, DK), position)
    retained = retention(queries, keys_turned, value_rows.reshape(SEQUENCE_LENGTH, RETENTION_HEADS, DV), log_decay)
    scaled = retained * lax.rsqrt(lax.optimization_barrier(jnp.mean(retained * retained, axis=-1, keepdims=True)) + epsilon)
    gate_wide = gate_rows.astype(jnp.float32).reshape(SEQUENCE_LENGTH, RETENTION_HEADS, DV)
    gated = (jax.nn.silu(gate_wide) * scaled).astype(jnp.bfloat16).reshape(SEQUENCE_LENGTH, RETENTION_HEADS * DV)
    mixer_out = blocked_product(gated, out_weight, N_TP).astype(jnp.bfloat16)
    widened = channel_input.astype(jnp.float32)
    normed = (widened * lax.rsqrt(lax.optimization_barrier(jnp.mean(widened * widened, axis=-1, keepdims=True)) + epsilon) * norm_gain).astype(jnp.bfloat16)
    shared_result = blocked_product(swiglu_hidden(normed, shared_gate, shared_up), shared_down, N_TP)
    flat_expert = routes.reshape(-1)
    assign_count = flat_expert.shape[0]
    flat_token = jnp.arange(assign_count, dtype=jnp.int32) // TOPK
    flat_weight = route_weight.reshape(-1)
    limit = N_EP * N_TP * CAP

    def add_expert(total, expert):
        chosen = jnp.nonzero(flat_expert == expert, size=limit, fill_value=assign_count)[0].astype(jnp.int32)
        valid = chosen < assign_count
        safe = jnp.minimum(chosen, assign_count - 1)
        token_index = flat_token[safe]
        weight = jnp.where(valid, flat_weight[safe], 0.0)
        hidden = swiglu_hidden(normed[token_index], expert_gate[expert], expert_up[expert])
        result = blocked_product(hidden, expert_down[expert], N_TP).astype(jnp.bfloat16)
        result = lax.optimization_barrier(result)
        return (total.at[token_index].add(weight[:, None] * result.astype(jnp.float32)), None)
    routed, _ = lax.scan(add_expert, jnp.zeros((TOKENS_M, D), jnp.float32), jnp.arange(EXPERTS, dtype=jnp.int32))
    channel_out = (shared_result + routed).astype(jnp.bfloat16)
    return (mixer_out, channel_out)
```

```python
import functools

import jax
import jax.numpy as jnp
import numpy as np
from jax import lax
from jax.experimental import pallas as pl
from jax.experimental.pallas import tpu as pltpu
from jax.sharding import Mesh
from jax.sharding import PartitionSpec as P

EP = ("y", "x")
TP = ("z", "c")
ALL = ("y", "x", "z", "c")
MESH = pl.DeviceIdType.MESH
F32 = jnp.float32
BF16 = jnp.bfloat16
epsilon = 1e-06
turn_base = 10000.0

D = 2048
NE = 16
NZ = 8
BLOCK = 128
CAP = 5
TM = 48
PAIR = 2 * CAP
ROWS = NE * PAIR
HALF = ROWS // 2
PAD = 16
RET = 32
CO, CM, CR0, CR1 = 0, 1, 2, 3


def dot(a, b, dims=None, precision=None):
    if dims is None:
        return jnp.dot(a, b, preferred_element_type=F32, precision=precision)
    return lax.dot_general(a, b, (dims, ((), ())), preferred_element_type=F32)


def silu(v):
    return v / (1.0 + jnp.exp(-v))


def constants():
    place = np.zeros((2, NE * PAD, 128), np.float32)
    comb = np.zeros((3, 2, 128, NE * RET), np.float32)
    select = np.zeros((ROWS, NE * PAD), np.float32)
    perm = np.zeros((NE * RET, 3 * ROWS), np.float32)
    for j in range(NE):
        for rel in range(2):
            for p in range(CAP):
                place[rel, j * PAD + rel * CAP + p, j * CAP + p] = 1
                for zi in range(3):
                    comb[zi, rel, j * CAP + p, j * RET + zi * PAIR + rel * CAP + p] = 1
        for r in range(PAIR):
            select[j * PAIR + r, j * PAD + r] = 1
            for zi in range(3):
                perm[j * RET + zi * PAIR + r, zi * ROWS + j * PAIR + r] = 1
    return [jnp.asarray(m, BF16) for m in (place, comb, select, perm)]


def kernel(
    q_ref, k_ref, v_ref, g_ref, decay_ref, ow_ref, normed_ref, meta_ref,
    eg_ref, eu_ref, ed_ref, sg_ref, su_ref, sd_ref,
    cplace_ref, ccomb_ref, cselect_ref, cperm_ref,
    mixer_ref, channel_ref,
    wr, wd, ws, wsd, pn, pm, outg, a2a, ag_o, ag_m, ag_r, hid, ret_s, ret_r,
    acc, oth, othp, mix, mixp, rs_s, rs_r, rm_s, rm_r,
    st_s, st_r, before, state, entry, run_s, off_s,
    load_sem, w_s, w_r, pair_s, pair_r, a2a_s, a2a_r, ag_s, ag_v, st_ss, st_rs,
    ret_ss, ret_rs, oth_s, oth_r, mixp_s, mixp_r, rs_ss, rs_rs, rm_ss, rm_rs,
):
    y, x, z, c = (lax.axis_index(a) for a in ALL)
    me = y * 4 + x
    pc = 1 - c
    zup, zdown = lax.rem(z + 1, NZ), lax.rem(z + NZ - 1, NZ)
    partner = {"c": pc}

    def zat(offset):
        return lax.rem(z + (offset + NZ), NZ)

    def peer(j):
        return {"y": lax.div(j, 4), "x": lax.rem(j, 4)}

    def rcopy(src, dst, ss, rs, dev):
        return pltpu.make_async_remote_copy(
            src_ref=src, dst_ref=dst, send_sem=ss, recv_sem=rs, device_id=dev, device_id_type=MESH
        )

    barrier = pltpu.get_barrier_semaphore()
    for k in range(1, NE):
        pl.semaphore_signal(
            barrier, inc=1, device_id=peer(lax.rem(me + k, NE)), device_id_type=MESH
        )
    for dev in ({"z": zup}, {"z": zdown}, partner):
        pl.semaphore_signal(barrier, inc=1, device_id=dev, device_id_type=MESH)
    pl.semaphore_wait(barrier, NE + 2)

    pair = [
        rcopy(normed_ref, pn, pair_s.at[0], pair_r.at[0], partner),
        rcopy(meta_ref.at[pc], pm.at[0], pair_s.at[1], pair_r.at[1], partner),
        rcopy(meta_ref.at[2 + pc], pm.at[1], pair_s.at[2], pair_r.at[2], partner),
    ]
    for copy in pair:
        copy.start()

    def ag_copy(way, hop, chunk, src_z, first=False):
        buf = {CO: ag_o.at[src_z], CM: ag_m.at[src_z]}.get(chunk)
        if buf is None:
            buf = ag_r.at[src_z, chunk - CR0]
        src = normed_ref if first and chunk == CO else buf
        dev = {"z": zup if way == 0 else zdown}
        return rcopy(src, buf, ag_s.at[way, hop, chunk], ag_v.at[way, hop, chunk], dev)

    def ag_start(way, hop, chunk):
        ag_copy(way, hop, chunk, zat(-hop if way == 0 else hop)).start()

    def ag_wait(way, hop, chunk):
        ag_copy(way, hop, chunk, zat(-(hop + 1) if way == 0 else hop + 1)).wait_recv()

    for way in (0, 1):
        ag_copy(way, 0, CO, z, first=True).start()
    weights = [
        (eg_ref.at[pc], wr.at[1, :, pl.ds(0, 128)]),
        (eu_ref.at[pc], wr.at[1, :, pl.ds(128, 128)]),
        (ed_ref.at[pc], wd.at[pl.ds(128, 128)]),
        (sg_ref, ws.at[1, :, pl.ds(0, 128)]),
        (su_ref, ws.at[1, :, pl.ds(128, 128)]),
        (sd_ref, wsd.at[pl.ds(128, 128)]),
    ]
    sent = [rcopy(s, d, w_s.at[n], w_r.at[n], partner) for n, (s, d) in enumerate(weights)]
    loads = [
        (eg_ref.at[c], wr.at[0, :, pl.ds(0, 128)]),
        (eu_ref.at[c], wr.at[0, :, pl.ds(128, 128)]),
        (ed_ref.at[c], wd.at[pl.ds(0, 128)]),
        (sg_ref, ws.at[0, :, pl.ds(0, 128)]),
        (su_ref, ws.at[0, :, pl.ds(128, 128)]),
        (sd_ref, wsd.at[pl.ds(0, 128)]),
    ]
    loaded = [pltpu.make_async_copy(s, d, load_sem.at[n]) for n, (s, d) in enumerate(loads)]
    for copy in sent + loaded:
        copy.start()
    ag_o[z] = normed_ref[...]
    ag_m[z, pl.ds(0, TM)] = meta_ref[2 + c]
    for copy in pair:
        copy.wait_recv()
    ag_m[z, pl.ds(TM, TM)] = pm[1]
    for way in (0, 1):
        ag_start(way, 0, CM)

    def wide(count, body):
        def step(n, carry):
            body(pl.ds(pl.multiple_of(n * (D // count), D // count), D // count))
            return carry

        lax.fori_loop(0, count, step, 0)

    own_pick = dot(cplace_ref[0], meta_ref[c], ((1,), (1,))).astype(BF16)
    other_pick = dot(cplace_ref[1], pm[0], ((1,), (1,))).astype(BF16)

    def gather_rows(cols):
        rows = dot(own_pick, normed_ref[:, cols]) + dot(other_pick, pn[:, cols])
        outg[:, :, cols] = rows.astype(BF16).reshape(NE, PAD, D // 4)

    wide(4, gather_rows)

    def a2a_copy(j, slot):
        return rcopy(outg.at[j], a2a.at[slot], a2a_s.at[j], a2a_r.at[slot], peer(j))

    def over_peers(body):
        def step(k, carry):
            body(lax.rem(me + k, NE))
            return carry

        lax.fori_loop(1, NE, step, 0)

    over_peers(lambda j: a2a_copy(j, me).start())
    a2a[me] = outg[me]

    rows_i = lax.broadcasted_iota(jnp.int32, (BLOCK, BLOCK), 0)
    cols_i = lax.broadcasted_iota(jnp.int32, (BLOCK, BLOCK), 1)
    upper = (rows_i <= cols_i).astype(F32)
    lower = rows_i >= cols_i
    run_s[...] = dot(decay_ref[...], upper, precision=lax.Precision.HIGHEST)
    state[...] = jnp.zeros_like(state)

    def along(row):
        return jnp.transpose(jnp.broadcast_to(row, (BLOCK, BLOCK)))

    def local_state(n, total):
        rows = pl.ds(pl.multiple_of(n * BLOCK, BLOCK), BLOCK)
        row = run_s[pl.ds(n, 1), :]
        end = row[:, BLOCK - 1 :]
        off_s[pl.ds(n, 1), :] = jnp.broadcast_to(total, (1, BLOCK))
        tail = jnp.exp(end - along(row))
        keyed = (k_ref[rows, :].astype(F32) * tail).astype(BF16)
        before[n] = state[...]
        state[...] = jnp.exp(end) * state[...] + dot(keyed, v_ref[rows, :], ((0,), (0,)))
        return total + end

    total = lax.fori_loop(0, NZ, local_state, jnp.zeros((1, 1), F32))
    st_s[pl.ds(0, BLOCK), :] = state[...].astype(BF16)
    high = total.astype(BF16).astype(F32)
    middle = (total - high).astype(BF16).astype(F32)
    low = total - high - middle
    line = lax.broadcasted_iota(jnp.int32, (16, 256), 0)
    pieces = jnp.where(line == 0, high, jnp.where(line == 1, middle, jnp.where(line == 2, low, 0.0)))
    st_s[pl.ds(BLOCK, 16), :] = pieces.astype(BF16)

    def st_copy(j, slot):
        return rcopy(st_s, st_r.at[slot], st_ss.at[j], st_rs.at[slot], peer(j))

    def each_later(body):
        def step(j, carry):
            @pl.when(j > me)
            def _():
                body(j)

            return carry

        lax.fori_loop(1, NE, step, 0)

    each_later(lambda j: st_copy(j, me).start())

    over_peers(lambda j: a2a_copy(j, j).wait_recv())

    def pack_rows(cols):
        rows = dot(cselect_ref[...], a2a[:, :, cols].reshape(NE * PAD, D // 4))
        ag_r[z, :, :, cols] = rows.astype(BF16).reshape(2, HALF, D // 4)

    wide(4, pack_rows)
    for chunk in (CR0, CR1):
        for way in (0, 1):
            ag_start(way, 0, chunk)
    for chunk in (CO, CM):
        for way in (0, 1):
            ag_wait(way, 0, chunk)
            ag_start(way, 1, chunk)
    for copy in loaded:
        copy.wait()
    for copy in sent:
        copy.wait_recv()

    def hidden(rows, weight):
        parts = []
        for n in (0, 1):
            both = dot(rows, weight[n])
            parts.append((silu(both[:, :128]) * both[:, 128:]).astype(BF16))
        return jnp.concatenate(parts, axis=1)

    def shared(za, zb=None):
        rows = ag_o[za] if zb is None else jnp.concatenate([ag_o[za], ag_o[zb]], axis=0)
        h = hidden(rows, ws)

        def down(cols):
            result = dot(h, wsd[:, cols])
            acc[za, :, cols] = result[:TM]
            if zb is not None:
                acc[zb, :, cols] = result[TM:]

        wide(4, down)

    hid[2] = hidden(ag_r[z].reshape(ROWS, D), wr)
    shared(z)

    entry[...] = jnp.zeros_like(entry)

    def take_state(j, carry):
        @pl.when(j < me)
        def _():
            st_copy(j, j).wait_recv()
            sums = st_r[j, pl.ds(BLOCK, 16), :].astype(F32)
            decay = jnp.exp(sums[0:1] + sums[1:2] + sums[2:3])
            entry[...] = decay * entry[...] + st_r[j, pl.ds(0, BLOCK), :].astype(F32)

        return carry

    lax.fori_loop(0, NE - 1, take_state, 0)

    def retain(n, carry):
        rows = pl.ds(pl.multiple_of(n * BLOCK, BLOCK), BLOCK)
        row = run_s[pl.ds(n, 1), :]
        spread = along(row)
        query, key, value = q_ref[rows, :], k_ref[rows, :], v_ref[rows, :]
        scores = dot(query, key, ((1,), (1,)))
        factor = jnp.exp(jnp.where(lower, spread - row, 0.0))
        mixed = jnp.where(lower, scores * factor, 0.0).astype(BF16)
        scaled_query = (query.astype(F32) * jnp.exp(spread)).astype(BF16)
        offset = jnp.exp(off_s[pl.ds(n, 1), :][:, 0:1])
        prior = (before[n] + offset * entry[...]).astype(BF16)
        kept = dot(mixed, value) + dot(scaled_query, prior)
        scale = lax.rsqrt(jnp.mean(kept * kept, axis=-1, keepdims=True) + epsilon)
        gated = (silu(g_ref[rows, :].astype(F32)) * (kept * scale)).astype(BF16)

        def project(cols):
            term = dot(gated, ow_ref[:, cols]).astype(BF16)
            mix[0, n, :, cols] = term[:64]
            mix[1, n, :, cols] = term[64:]

        wide(4, project)
        return carry

    lax.fori_loop(0, NZ, retain, 0)
    mix_copy = rcopy(mix.at[pc], mixp, mixp_s, mixp_r, partner)
    mix_copy.start()

    def ret_copy(g, j, slot):
        return rcopy(
            ret_s.at[g, j], ret_r.at[g, slot], ret_ss.at[g, j], ret_rs.at[g, slot], peer(j)
        )

    def far(hop, chunk):
        if chunk in (CO, CR0):
            ag_start(0, hop, chunk)
        else:
            ag_start(1, hop, chunk)

    def hop_step(h, carry):
        za, zb = zat(-h), zat(h)
        for k in (0, 1):
            for way in (0, 1):
                ag_wait(way, h - 1, CR0 + k)

            @pl.when(h < 3)
            def _():
                for way in (0, 1):
                    ag_start(way, h, CR0 + k)

            @pl.when(h == 3)
            def _():
                far(3, CR0 + k)

            if k == 0:

                @pl.when(h > 1)
                def _():
                    for chunk in (CO, CM):
                        for way in (0, 1):
                            ag_wait(way, h - 1, chunk)

                @pl.when(h == 2)
                def _():
                    for chunk in (CO, CM):
                        for way in (0, 1):
                            ag_start(way, 2, chunk)

                @pl.when(h == 3)
                def _():
                    for chunk in (CO, CM):
                        far(3, chunk)

            h_rows = hidden(jnp.concatenate([ag_r[za, k], ag_r[zb, k]], axis=0), wr)
            hid[0, pl.ds(k * HALF, HALF)] = h_rows[:HALF]
            hid[1, pl.ds(k * HALF, HALF)] = h_rows[HALF:]
        shared(za, zb)

        @pl.when(h == 3)
        def _():
            ag_wait(0, 3, CR0)
            ag_wait(1, 3, CR1)
            ag_wait(0, 3, CO)
            ag_wait(1, 3, CM)
            hid[2] = hidden(ag_r[zat(4)].reshape(ROWS, D), wr)
            shared(zat(4))

        g = h - 1
        placed = dot(cperm_ref[...], hid[...].reshape(3 * ROWS, 256)).astype(BF16)

        def down(cols):
            result = dot(placed, wd[:, cols]).astype(BF16)
            ret_s[g, :, :, cols] = result.reshape(NE, RET, D // 8)

        wide(8, down)
        over_peers(lambda j: ret_copy(g, j, me).start())
        ret_r[g, me] = ret_s[g, me]
        return carry

    lax.fori_loop(1, 4, hop_step, 0)

    def chain(base, send, recv, ss, rs, rows):
        def copy(way, s):
            dev = {"z": zup if way == 0 else zdown}
            src, dst = send.at[way, s], recv.at[way, s]
            if s == 0:
                cols = pl.ds(way * (D // 2), D // 2)
                src, dst = src.at[:, cols], dst.at[:, cols]
            return rcopy(src, dst, ss.at[way, s], rs.at[way, s], dev)

        def step(s):
            for way in (0, 1):
                target = zat(4 - s if way == 0 else s - 4)
                if s == 0:
                    cols = pl.ds(way * (D // 2), D // 2)
                    send[way, s, :, cols] = base(target, cols).astype(BF16)
                else:
                    copy(way, s - 1).wait_recv()
                    for part in (0, 1):
                        cols = pl.ds(part * (D // 2), D // 2)
                        value = base(target, cols)
                        if s > 1 or part == way:
                            value = value + recv[way, s - 1, :, cols].astype(F32)
                        send[way, s, :, cols] = value.astype(BF16)
                copy(way, s).start()

        def finish(out_ref):
            for way in (0, 1):
                copy(way, 3).wait_recv()
            for part in (0, 1):
                cols = pl.ds(part * (D // 2), D // 2)
                value = base(z, cols)
                for way in (0, 1):
                    value = value + recv[way, 3, :, cols].astype(F32)
                out_ref[:, cols] = value.astype(BF16)

        def drain():
            for way in (0, 1):
                for s in range(4):
                    copy(way, s).wait_send()

        return step, finish, drain

    def mix_base(target, cols):
        return mix[c, target, :, cols].astype(F32) + mixp[target, :, cols].astype(F32)

    def moe_base(target, cols):
        return acc[target, :, cols] + othp[target, :, cols].astype(F32)

    mix_step, mix_finish, mix_drain = chain(mix_base, rm_s, rm_r, rm_ss, rm_rs, 64)
    moe_step, moe_finish, moe_drain = chain(moe_base, rs_s, rs_r, rs_ss, rs_rs, TM)

    sources = [(0, 0, -1), (0, 1, 1), (0, 2, 0), (1, 0, -2), (1, 1, 2), (2, 0, -3), (2, 1, 3), (2, 2, 4)]

    def oth_copy(n):
        where = zat(sources[n][2])
        return rcopy(oth.at[where], othp.at[where], oth_s.at[n], oth_r.at[n], partner)

    def combine(g):
        over_peers(lambda j: ret_copy(g, j, j).wait_recv())
        for n, (group, zi, offset) in enumerate(sources):
            if group != g:
                continue
            where = zat(offset)
            weight = ag_m[where]
            spread = jnp.concatenate(
                [dot(weight[:TM], ccomb_ref[zi, 0]), dot(weight[TM:], ccomb_ref[zi, 1])], axis=0
            ).astype(BF16)

            def gather(cols):
                result = dot(spread, ret_r[g, :, :, cols].reshape(NE * RET, D // 4))
                acc[where, :, cols] += result[:TM]
                oth[where, :, cols] = result[TM:].astype(BF16)

            wide(4, gather)
            oth_copy(n).start()

    mix_copy.wait_recv()
    mix_step(0)
    combine(0)
    mix_step(1)
    combine(1)
    mix_step(2)
    mix_step(3)
    combine(2)
    for n in range(NZ):
        oth_copy(n).wait_recv()
    moe_step(0)
    mix_finish(mixer_ref)
    for s in (1, 2, 3):
        moe_step(s)
    moe_finish(channel_ref)

    for copy in pair + sent + [mix_copy]:
        copy.wait_send()
    over_peers(lambda j: a2a_copy(j, me).wait_send())
    each_later(lambda j: st_copy(j, me).wait_send())
    for way in (0, 1):
        ag_copy(way, 0, CO, z, first=True).wait_send()
        for hop in range(3):
            for chunk in (CO, CM, CR0, CR1):
                if hop or chunk != CO:
                    ag_copy(way, hop, chunk, z).wait_send()
    for way, chunk in ((0, CO), (1, CM), (0, CR0), (1, CR1)):
        ag_copy(way, 3, chunk, z).wait_send()
    for g in range(3):
        over_peers(lambda j: ret_copy(g, j, me).wait_send())
    for n in range(NZ):
        oth_copy(n).wait_send()
    mix_drain()
    moe_drain()


def fused(*args):
    vmem = pl.BlockSpec(memory_space=pltpu.VMEM)
    hbm = pl.BlockSpec(memory_space=pl.ANY)
    sem = pltpu.SemaphoreType.DMA
    scratch = [
        pltpu.VMEM(s, t)
        for s, t in (
            ((2, D, 256), BF16), ((256, D), BF16), ((2, D, 256), BF16), ((256, D), BF16),
            ((TM, D), BF16), ((2, TM, 128), BF16),
            ((NE, PAD, D), BF16), ((NE, PAD, D), BF16),
            ((NZ, TM, D), BF16), ((NZ, 2 * TM, 128), BF16), ((NZ, 2, HALF, D), BF16),
            ((3, ROWS, 256), BF16),
            ((3, NE, RET, D), BF16), ((3, NE, RET, D), BF16),
            ((NZ, TM, D), F32), ((NZ, TM, D), BF16), ((NZ, TM, D), BF16),
            ((2, NZ, 64, D), BF16), ((NZ, 64, D), BF16),
            ((2, 4, TM, D), BF16), ((2, 4, TM, D), BF16),
            ((2, 4, 64, D), BF16), ((2, 4, 64, D), BF16),
            ((144, 256), BF16), ((NE, 144, 256), BF16),
            ((NZ, BLOCK, 256), F32), ((BLOCK, 256), F32), ((BLOCK, 256), F32),
            ((NZ, BLOCK), F32), ((NZ, BLOCK), F32),
        )
    ] + [
        sem((6,)), sem((6,)), sem((6,)), sem((3,)), sem((3,)), sem((NE,)), sem((NE,)),
        sem((2, 4, 4)), sem((2, 4, 4)), sem((NE,)), sem((NE,)),
        sem((3, NE)), sem((3, NE)), sem((NZ,)), sem((NZ,)), sem, sem,
        sem((2, 4)), sem((2, 4)), sem((2, 4)), sem((2, 4)),
    ]
    return pl.pallas_call(
        kernel,
        out_shape=(jax.ShapeDtypeStruct((64, D), BF16), jax.ShapeDtypeStruct((TM, D), BF16)),
        in_specs=[vmem] * 8 + [hbm] * 6 + [vmem] * 4,
        out_specs=(vmem, vmem),
        scratch_shapes=scratch,
        compiler_params=pltpu.CompilerParams(
            collective_id=0, has_side_effects=True, vmem_limit_bytes=67043328
        ),
    )(*args)


def turn(rows, position):
    half = rows.shape[-1] // 2
    inverse = turn_base ** (-jnp.arange(half, dtype=F32) / half)
    angles = position[:, None] * inverse[None, :]
    cosine, sine = jnp.cos(angles), jnp.sin(angles)
    wide = rows.astype(F32)
    first, second = wide[:, :half], wide[:, half:]
    return jnp.concatenate(
        [first * cosine - second * sine, second * cosine + first * sine], axis=-1
    ).astype(BF16)


def routing(routes, route_weight, expert_count):
    flat = routes.reshape(-1)
    onehot = (flat[:, None] == jnp.arange(expert_count, dtype=jnp.int32)[None, :]).astype(BF16)
    count = flat.shape[0]
    strict = jnp.asarray(np.tril(np.ones((count, count), np.float32), -1), BF16)
    earlier = jnp.dot(strict, onehot, preferred_element_type=F32)
    rank = jnp.sum(earlier * onehot.astype(F32), axis=1).astype(jnp.int32).reshape(routes.shape)
    lane = (routes // 2) * CAP + rank
    hit = (lane[:, :, None] == jnp.arange(128, dtype=jnp.int32)).astype(F32)
    parity = (routes[:, :, None] % 2) == jnp.arange(2, dtype=jnp.int32)
    share = parity.astype(F32)
    place = jnp.einsum("nkl,nke->enl", hit, share)
    comb = jnp.einsum("nkl,nke->enl", hit * route_weight[:, :, None], share)
    return jnp.concatenate([place, comb], axis=0).astype(BF16)


def local(
    query_rows, key_rows, value_rows, gate_rows, log_decay, out_weight, channel_input, norm_gain,
    routes, route_weight, expert_gate, expert_up, expert_down, shared_gate, shared_up, shared_down,
):
    tokens = query_rows.shape[0]
    position = (lax.axis_index(EP) * tokens + jnp.arange(tokens, dtype=jnp.int32)).astype(F32)
    queries = turn(query_rows, position)
    keys = turn(key_rows, position)
    wide = channel_input.astype(F32)
    normed = (
        wide * lax.rsqrt(jnp.mean(wide * wide, axis=-1, keepdims=True) + epsilon) * norm_gain
    ).astype(BF16)
    meta = routing(routes, route_weight, 2 * NE)
    return fused(
        queries, keys, value_rows, gate_rows, log_decay.reshape(NZ, BLOCK), out_weight, normed,
        meta, expert_gate, expert_up, expert_down, shared_gate, shared_up, shared_down,
        *constants(),
    )


def solution(mesh):
    split = Mesh(mesh.devices.reshape(4, 4, NZ, 2), ALL)
    return jax.shard_map(
        local,
        mesh=split,
        in_specs=(
            P(EP, TP), P(EP, TP), P(EP, TP), P(EP, TP), P(TP, EP), P(TP, None),
            P(ALL, None), P(), P(ALL, None), P(ALL, None),
            P(EP, None, TP), P(EP, None, TP), P(EP, TP, None),
            P(None, TP), P(None, TP), P(TP, None),
        ),
        out_specs=(P(ALL, None), P(ALL, None)),
        check_vma=False,
    )
```

```python
import functools

import jax
import jax.numpy as jnp
import numpy as np
from jax import lax
from jax.experimental import pallas as pl
from jax.experimental.pallas import tpu as pltpu
from jax.sharding import Mesh
from jax.sharding import PartitionSpec as P

EP = ("y", "x")
TP = ("z", "c")
ALL = ("y", "x", "z", "c")
MESH = pl.DeviceIdType.MESH
F32 = jnp.float32
BF16 = jnp.bfloat16
epsilon = 1e-06
turn_base = 10000.0

D = 2048
NE = 16
NZ = 8
BLOCK = 128
CAP = 5
TM = 48
PAIR = 2 * CAP
ROWS = NE * PAIR
HALF = ROWS // 2
PAD = 16
RET = 32
CO, CM, CR0, CR1 = 0, 1, 2, 3
SENT = (16, 24, 24, 32)
ORDER = (
    (2, 2), (3, 2), (2, 3), (1, 2), (2, 1), (2, 0), (0, 2), (3, 1), (1, 3), (3, 3), (1, 1),
    (3, 0), (0, 3), (1, 0), (0, 1),
)


def dot(a, b, dims=None, precision=None):
    if dims is None:
        return jnp.dot(a, b, preferred_element_type=F32, precision=precision)
    return lax.dot_general(a, b, (dims, ((), ())), preferred_element_type=F32)


def silu(v):
    return v / (1.0 + jnp.exp(-v))


def constants():
    place = np.zeros((2, NE * PAD, 128), np.float32)
    comb = np.zeros((3, 2, 128, NE * RET), np.float32)
    comb_own = np.zeros((2, 128, NE * PAD), np.float32)
    select = np.zeros((ROWS, NE * PAD), np.float32)
    perm = np.zeros((NE * RET, 3 * ROWS), np.float32)
    for j in range(NE):
        for rel in range(2):
            for p in range(CAP):
                comb_own[rel, j * CAP + p, j * PAD + rel * CAP + p] = 1
                place[rel, j * PAD + rel * CAP + p, j * CAP + p] = 1
                for zi in range(3):
                    comb[zi, rel, j * CAP + p, j * RET + zi * PAIR + rel * CAP + p] = 1
        for r in range(PAIR):
            select[j * PAIR + r, j * PAD + r] = 1
            for zi in range(3):
                perm[j * RET + zi * PAIR + r, zi * ROWS + j * PAIR + r] = 1
    rate = turn_base ** (-(np.arange(128) % 64) / 64.0)
    near = np.arange(BLOCK)[:, None] * rate
    far = np.arange(128)[:, None] * float(BLOCK) * rate
    turns = np.stack([np.cos(near), np.sin(near), np.cos(far), np.sin(far)])
    tables = [jnp.asarray(m, BF16) for m in (place, comb, comb_own, select, perm)]
    return tables + [jnp.asarray(turns, F32)]


def kernel(
    chan_ref, gain_ref, routes_ref, share_ref,
    q_hbm, k_hbm, v_hbm, g_hbm, decay_hbm, ow_hbm,
    eg_ref, eu_ref, ed_ref, sg_ref, su_ref, sd_ref,
    cplace_hbm, ccomb_hbm, ccomb0_hbm, cselect_hbm, cperm_hbm, turns_hbm,
    mixer_ref, channel_ref,
    q_ref, k_ref, v_ref, g_ref, decay_ref, ow_ref,
    cplace_ref, ccomb_ref, ccomb0_ref, cselect_ref, cperm_ref, turns_ref, normed_ref, meta_ref, keys,
    wr, wd, ws, wsd, pn, pm, outg, a2a, ag_o, ag_m, ag_r, hid, ret_s, ret_r,
    acc, oth, othp, mix, mixp, rs_s, rs_r, rm_s, rm_r,
    st_s, st_r, before, state, entry, run_s, off_s,
    in_sem, load_sem, w_s, w_r, pair_s, pair_r, a2a_s, a2a_r, ag_s, ag_v, st_ss, st_rs,
    ret_ss, ret_rs, oth_s, oth_r, mixp_s, mixp_r, rs_ss, rs_rs, rm_ss, rm_rs,
):
    y, x, z, c = (lax.axis_index(a) for a in ALL)
    me = y * 4 + x
    pc = 1 - c
    zup, zdown = lax.rem(z + 1, NZ), lax.rem(z + NZ - 1, NZ)
    partner = {"c": pc}

    def zat(offset):
        return lax.rem(z + (offset + NZ), NZ)

    def peer(j):
        return {"y": lax.div(j, 4), "x": lax.rem(j, 4)}

    others = [lax.rem(y + dy, 4) * 4 + lax.rem(x + dx, 4) for dy, dx in ORDER]

    def over_peers(body):
        for j in others:
            body(j)

    def rcopy(src, dst, ss, rs, dev):
        return pltpu.make_async_remote_copy(
            src_ref=src, dst_ref=dst, send_sem=ss, recv_sem=rs, device_id=dev, device_id_type=MESH
        )

    for g in (1, 2):
        ret_r[g, :, pl.ds(16, 16), :] = jnp.zeros((NE, 16, D), BF16)
    barrier = pltpu.get_barrier_semaphore()
    for j in others:
        pl.semaphore_signal(barrier, inc=1, device_id=peer(j), device_id_type=MESH)
    for dev in ({"z": zup}, {"z": zdown}, partner):
        pl.semaphore_signal(barrier, inc=1, device_id=dev, device_id_type=MESH)
    incoming = [
        (cplace_hbm, cplace_ref), (k_hbm, k_ref), (v_hbm, v_ref), (decay_hbm, decay_ref),
        (turns_hbm, turns_ref), (cselect_hbm, cselect_ref), (q_hbm, q_ref), (g_hbm, g_ref),
        (ow_hbm, ow_ref), (cperm_hbm, cperm_ref), (ccomb0_hbm, ccomb0_ref), (ccomb_hbm, ccomb_ref),
    ]
    arriving = [pltpu.make_async_copy(s, d, in_sem.at[n]) for n, (s, d) in enumerate(incoming)]
    for copy in arriving:
        copy.start()

    wide_rows = chan_ref[...].astype(F32)
    mean = jnp.mean(wide_rows * wide_rows, axis=-1, keepdims=True)
    normed_ref[...] = (wide_rows * lax.rsqrt(mean + epsilon) * gain_ref[...]).astype(BF16)
    lanes = lax.broadcasted_iota(jnp.int32, (TM, 128), 1)
    picks = [routes_ref[:, k : k + 1] for k in (0, 1)]
    hits = [(lanes == pick).astype(F32) for pick in picks]
    strict = lax.broadcasted_iota(jnp.int32, (TM, TM), 0) > lax.broadcasted_iota(
        jnp.int32, (TM, TM), 1
    )
    earlier = dot(strict.astype(F32).astype(BF16), (hits[0] + hits[1]).astype(BF16))
    metas = [jnp.zeros((TM, 128), F32)] * 4
    for k in (0, 1):
        rank = jnp.sum(earlier * hits[k], axis=-1, keepdims=True)
        slot = (picks[k] >> 1).astype(F32) * CAP + rank
        there = (lanes.astype(F32) == slot).astype(F32)
        for parity in (0, 1):
            mine = there * ((picks[k] & 1) == parity).astype(F32)
            metas[parity] += mine
            metas[2 + parity] += mine * share_ref[:, k : k + 1]
    for n in range(4):
        meta_ref[n] = metas[n].astype(BF16)
    pl.semaphore_wait(barrier, NE + 2)

    pair = [
        rcopy(normed_ref, pn, pair_s.at[0], pair_r.at[0], partner),
        rcopy(meta_ref.at[pc], pm.at[0], pair_s.at[1], pair_r.at[1], partner),
        rcopy(meta_ref.at[2 + pc], pm.at[1], pair_s.at[2], pair_r.at[2], partner),
    ]
    for copy in pair:
        copy.start()

    def ag_copy(way, hop, chunk, src_z, first=False):
        buf = {CO: ag_o.at[src_z], CM: ag_m.at[src_z]}.get(chunk)
        if buf is None:
            buf = ag_r.at[src_z, chunk - CR0]
        src = normed_ref if first and chunk == CO else buf
        dev = {"z": zup if way == 0 else zdown}
        return rcopy(src, buf, ag_s.at[way, hop, chunk], ag_v.at[way, hop, chunk], dev)

    def ag_start(way, hop, chunk):
        ag_copy(way, hop, chunk, zat(-hop if way == 0 else hop)).start()

    def ag_wait(way, hop, chunk):
        ag_copy(way, hop, chunk, zat(-(hop + 1) if way == 0 else hop + 1)).wait_recv()

    for way in (0, 1):
        ag_copy(way, 0, CO, z, first=True).start()
    weights = [
        (eg_ref.at[pc], wr.at[1, :, pl.ds(0, 128)]),
        (eu_ref.at[pc], wr.at[1, :, pl.ds(128, 128)]),
        (ed_ref.at[pc], wd.at[pl.ds(128, 128)]),
        (sg_ref, ws.at[1, :, pl.ds(0, 128)]),
        (su_ref, ws.at[1, :, pl.ds(128, 128)]),
        (sd_ref, wsd.at[pl.ds(128, 128)]),
    ]
    sent = [rcopy(s, d, w_s.at[n], w_r.at[n], partner) for n, (s, d) in enumerate(weights)]
    loads = [
        (eg_ref.at[c], wr.at[0, :, pl.ds(0, 128)]),
        (eu_ref.at[c], wr.at[0, :, pl.ds(128, 128)]),
        (ed_ref.at[c], wd.at[pl.ds(0, 128)]),
        (sg_ref, ws.at[0, :, pl.ds(0, 128)]),
        (su_ref, ws.at[0, :, pl.ds(128, 128)]),
        (sd_ref, wsd.at[pl.ds(0, 128)]),
    ]
    loaded = [pltpu.make_async_copy(s, d, load_sem.at[n]) for n, (s, d) in enumerate(loads)]
    for copy in sent + loaded:
        copy.start()
    ag_o[z] = normed_ref[...]
    ag_m[z, pl.ds(0, TM)] = meta_ref[2 + c]
    for copy in pair:
        copy.wait_recv()
    ag_m[z, pl.ds(TM, TM)] = pm[1]
    for way in (0, 1):
        ag_start(way, 0, CM)

    def wide(count, body):
        def step(n, carry):
            body(pl.ds(pl.multiple_of(n * (D // count), D // count), D // count))
            return carry

        lax.fori_loop(0, count, step, 0)

    arriving[0].wait()
    own_pick = dot(cplace_ref[0], meta_ref[c], ((1,), (1,))).astype(BF16)
    other_pick = dot(cplace_ref[1], pm[0], ((1,), (1,))).astype(BF16)

    def gather_rows(cols):
        rows = dot(own_pick, normed_ref[:, cols]) + dot(other_pick, pn[:, cols])
        outg[:, :, cols] = rows.astype(BF16).reshape(NE, PAD, D // 4)

    wide(4, gather_rows)

    def a2a_copy(j, slot):
        return rcopy(outg.at[j], a2a.at[slot], a2a_s.at[j], a2a_r.at[slot], peer(j))

    over_peers(lambda j: a2a_copy(j, me).start())
    a2a[me] = outg[me]

    def relay_own(hop):
        for chunk in (CO, CM):
            for way in (0, 1):
                ag_wait(way, hop, chunk)
        if hop < 2:
            for chunk in (CO, CM):
                for way in (0, 1):
                    ag_start(way, hop + 1, chunk)
        else:
            ag_start(0, 3, CO)
            ag_start(1, 3, CM)

    for copy in arriving[1:5]:
        copy.wait()
    half_lane = lax.broadcasted_iota(jnp.int32, (BLOCK, BLOCK), 1) < 64

    def turned(ref, n):
        rows = ref[pl.ds(pl.multiple_of(n * BLOCK, BLOCK), BLOCK), :].astype(F32)
        far_line = pl.ds(me * NZ + n, 1)
        near_cos, near_sin = turns_ref[0], turns_ref[1]
        far_cos, far_sin = turns_ref[2, far_line, :], turns_ref[3, far_line, :]
        cosine = far_cos * near_cos - far_sin * near_sin
        sine = far_sin * near_cos + far_cos * near_sin
        swapped = pltpu.roll(rows, 64, 1)
        return (rows * cosine + swapped * jnp.where(half_lane, -sine, sine)).astype(BF16)

    rows_i = lax.broadcasted_iota(jnp.int32, (BLOCK, BLOCK), 0)
    cols_i = lax.broadcasted_iota(jnp.int32, (BLOCK, BLOCK), 1)
    upper = (rows_i <= cols_i).astype(F32)
    lower = rows_i >= cols_i
    run_s[...] = dot(decay_ref[...], upper, precision=lax.Precision.HIGHEST)
    state[...] = jnp.zeros_like(state)

    def along(row):
        return jnp.transpose(jnp.broadcast_to(row, (BLOCK, BLOCK)))

    def local_state(n, total):
        rows = pl.ds(pl.multiple_of(n * BLOCK, BLOCK), BLOCK)
        row = run_s[pl.ds(n, 1), :]
        end = row[:, BLOCK - 1 :]
        off_s[pl.ds(n, 1), :] = jnp.broadcast_to(total, (1, BLOCK))
        tail = jnp.exp(end - along(row))
        key = turned(k_ref, n)
        keys[rows, :] = key
        keyed = (key.astype(F32) * tail).astype(BF16)
        before[n] = state[...]
        state[...] = jnp.exp(end) * state[...] + dot(keyed, v_ref[rows, :], ((0,), (0,)))
        return total + end

    total = lax.fori_loop(0, NZ, local_state, jnp.zeros((1, 1), F32))
    st_s[pl.ds(0, BLOCK), :] = state[...].astype(BF16)
    high = total.astype(BF16).astype(F32)
    middle = (total - high).astype(BF16).astype(F32)
    low = total - high - middle
    line = lax.broadcasted_iota(jnp.int32, (16, 256), 0)
    pieces = jnp.where(line == 0, high, jnp.where(line == 1, middle, jnp.where(line == 2, low, 0.0)))
    st_s[pl.ds(BLOCK, 16), :] = pieces.astype(BF16)

    def st_copy(j, slot):
        return rcopy(st_s, st_r.at[slot], st_ss.at[j], st_rs.at[slot], peer(j))

    def each_later(body):
        for j in others:

            @pl.when(j > me)
            def _():
                body(j)

    relay_own(0)
    relay_own(1)

    over_peers(lambda j: a2a_copy(j, j).wait_recv())
    each_later(lambda j: st_copy(j, me).start())
    arriving[5].wait()

    def pack_rows(cols):
        rows = dot(cselect_ref[...], a2a[:, :, cols].reshape(NE * PAD, D // 4))
        ag_r[z, :, :, cols] = rows.astype(BF16).reshape(2, HALF, D // 4)

    wide(4, pack_rows)
    for chunk in (CR0, CR1):
        for way in (0, 1):
            ag_start(way, 0, chunk)
    for copy in loaded + arriving[9:10]:
        copy.wait()
    for copy in sent:
        copy.wait_recv()

    def hidden(rows, weight):
        parts = []
        for n in (0, 1):
            both = dot(rows, weight[n])
            parts.append((silu(both[:, :128]) * both[:, 128:]).astype(BF16))
        return jnp.concatenate(parts, axis=1)

    def shared(za, zb=None):
        rows = ag_o[za] if zb is None else jnp.concatenate([ag_o[za], ag_o[zb]], axis=0)
        h = hidden(rows, ws)

        def down(cols):
            result = dot(h, wsd[:, cols])
            acc[za, :, cols] = result[:TM]
            if zb is not None:
                acc[zb, :, cols] = result[TM:]

        wide(4, down)

    def ret_copy(g, j, slot):
        rows = pl.ds(0, SENT[g])
        return rcopy(
            ret_s.at[g, j, rows], ret_r.at[g, slot, rows], ret_ss.at[g, j], ret_rs.at[g, slot],
            peer(j),
        )

    def give_back(g, placed):
        height = placed.shape[0] // NE

        def down(cols):
            result = dot(placed, wd[:, cols]).astype(BF16)
            ret_s[g, :, pl.ds(0, height), cols] = result.reshape(NE, height, D // 8)

        wide(8, down)
        over_peers(lambda j: ret_copy(g, j, me).start())
        ret_r[g, me] = ret_s[g, me]

    own_hidden = hidden(ag_r[z].reshape(ROWS, D), wr)
    give_back(0, dot(cselect_ref[...], own_hidden, ((0,), (0,))).astype(BF16))
    relay_own(2)
    shared(z)

    entry[...] = jnp.zeros_like(entry)

    def take_state(j, carry):
        @pl.when(j < me)
        def _():
            st_copy(j, j).wait_recv()
            sums = st_r[j, pl.ds(BLOCK, 16), :].astype(F32)
            decay = jnp.exp(sums[0:1] + sums[1:2] + sums[2:3])
            entry[...] = decay * entry[...] + st_r[j, pl.ds(0, BLOCK), :].astype(F32)

        return carry


    def retain(n, carry):
        rows = pl.ds(pl.multiple_of(n * BLOCK, BLOCK), BLOCK)
        row = run_s[pl.ds(n, 1), :]
        spread = along(row)
        query, key, value = turned(q_ref, n), keys[rows, :], v_ref[rows, :]
        scores = dot(query, key, ((1,), (1,)))
        factor = jnp.exp(jnp.where(lower, spread - row, 0.0))
        mixed = jnp.where(lower, scores * factor, 0.0).astype(BF16)
        scaled_query = (query.astype(F32) * jnp.exp(spread)).astype(BF16)
        offset = jnp.exp(off_s[pl.ds(n, 1), :][:, 0:1])
        prior = (before[n] + offset * entry[...]).astype(BF16)
        kept = dot(mixed, value) + dot(scaled_query, prior)
        scale = lax.rsqrt(jnp.mean(kept * kept, axis=-1, keepdims=True) + epsilon)
        gated = (silu(g_ref[rows, :].astype(F32)) * (kept * scale)).astype(BF16)

        def project(cols):
            term = dot(gated, ow_ref[:, cols]).astype(BF16)
            mix[0, n, :, cols] = term[:64]
            mix[1, n, :, cols] = term[64:]

        wide(4, project)
        return carry

    mix_copy = rcopy(mix.at[pc], mixp, mixp_s, mixp_r, partner)

    for h in (1, 2, 3):
        za, zb = zat(-h), zat(h)
        for k in (0, 1):
            for way in (0, 1):
                ag_wait(way, h - 1, CR0 + k)
            for way in (0, 1):
                if h < 3 or way == k:
                    ag_start(way, h, CR0 + k)
            h_rows = hidden(jnp.concatenate([ag_r[za, k], ag_r[zb, k]], axis=0), wr)
            hid[0, pl.ds(k * HALF, HALF)] = h_rows[:HALF]
            hid[1, pl.ds(k * HALF, HALF)] = h_rows[HALF:]
        if h < 3:
            placed = dot(cperm_ref[:, pl.ds(0, 2 * ROWS)], hid[pl.ds(0, 2)].reshape(2 * ROWS, 256))
        else:
            ag_wait(0, 3, CR0)
            ag_wait(1, 3, CR1)
            hid[2] = hidden(ag_r[zat(4)].reshape(ROWS, D), wr)
            placed = dot(cperm_ref[...], hid[...].reshape(3 * ROWS, 256))
        give_back(h, placed.astype(BF16))
        shared(za, zb)
        if h == 1:
            for copy in arriving[6:9]:
                copy.wait()
            lax.fori_loop(0, NE - 1, take_state, 0)
            lax.fori_loop(0, NZ // 2, retain, 0)
        if h == 2:
            lax.fori_loop(NZ // 2, NZ, retain, 0)
            mix_copy.start()
    ag_wait(0, 3, CO)
    ag_wait(1, 3, CM)
    shared(zat(4))

    def chain(base, send, recv, ss, rs):
        half = D // 2

        def copy(way, s, part):
            dev = {"z": zup if way == 0 else zdown}
            cols = pl.ds(part * half, half)
            return rcopy(
                send.at[way, s, :, cols], recv.at[way, s, :, cols], ss.at[way, s, part],
                rs.at[way, s, part], dev,
            )

        def forward(way, s, part):
            target = zat(4 - s if way == 0 else s - 4)
            cols = pl.ds(part * half, half)
            value = base(target, cols)
            if s > (0 if part == way else 1):
                copy(way, s - 1, part).wait_recv()
                value = value + recv[way, s - 1, :, cols].astype(F32)
            send[way, s, :, cols] = value.astype(BF16)
            copy(way, s, part).start()

        def step(s):
            for way in (0, 1):
                forward(way, s, way)
            if s < 3:
                for way in (0, 1):
                    forward(way, s + 1, 1 - way)

        def finish(out_ref):
            for part in (0, 1):
                cols = pl.ds(part * half, half)
                value = base(z, cols)
                for way in (0, 1):
                    copy(way, 3, part).wait_recv()
                    value = value + recv[way, 3, :, cols].astype(F32)
                out_ref[:, cols] = value.astype(BF16)

        def drain():
            for way in (0, 1):
                for s in range(4):
                    for part in (0, 1):
                        if s or part == way:
                            copy(way, s, part).wait_send()

        return step, finish, drain

    def mix_base(target, cols):
        return mix[c, target, :, cols].astype(F32) + mixp[target, :, cols].astype(F32)

    def moe_base(target, cols):
        return acc[target, :, cols] + othp[target, :, cols].astype(F32)

    mix_step, mix_finish, mix_drain = chain(mix_base, rm_s, rm_r, rm_ss, rm_rs)
    moe_step, moe_finish, moe_drain = chain(moe_base, rs_s, rs_r, rs_ss, rs_rs)

    sources = [
        (0, 0, 0), (1, 0, -1), (1, 1, 1), (2, 0, -2), (2, 1, 2), (3, 2, 4), (3, 0, -3), (3, 1, 3)
    ]

    def oth_copy(n):
        where = zat(sources[n][2])
        return rcopy(oth.at[where], othp.at[where], oth_s.at[n], oth_r.at[n], partner)

    def combine(g):
        over_peers(lambda j: ret_copy(g, j, j).wait_recv())
        for n, (group, zi, offset) in enumerate(sources):
            if group != g:
                continue
            where = zat(offset)
            weight = ag_m[where]
            table = [ccomb0_ref[rel] if g == 0 else ccomb_ref[zi, rel] for rel in (0, 1)]
            spread = jnp.concatenate(
                [dot(weight[:TM], table[0]), dot(weight[TM:], table[1])], axis=0
            ).astype(BF16)
            height = PAD if g == 0 else RET

            def gather(cols):
                rows = ret_r[g, :, pl.ds(0, height), cols].reshape(NE * height, D // 4)
                result = dot(spread, rows)
                acc[where, :, cols] += result[:TM]
                oth[where, :, cols] = result[TM:].astype(BF16)

            wide(4, gather)
            oth_copy(n).start()

    for copy in arriving[10:]:
        copy.wait()
    mix_copy.wait_recv()
    mix_step(0)
    combine(0)
    combine(1)
    mix_step(1)
    combine(2)
    mix_step(2)
    mix_step(3)
    combine(3)
    for n in range(NZ):
        oth_copy(n).wait_recv()
    moe_step(0)
    mix_finish(mixer_ref)
    for s in (1, 2, 3):
        moe_step(s)
    moe_finish(channel_ref)

    for copy in pair + sent + [mix_copy]:
        copy.wait_send()
    over_peers(lambda j: a2a_copy(j, me).wait_send())
    each_later(lambda j: st_copy(j, me).wait_send())
    for way in (0, 1):
        ag_copy(way, 0, CO, z, first=True).wait_send()
        for hop in range(3):
            for chunk in (CO, CM, CR0, CR1):
                if hop or chunk != CO:
                    ag_copy(way, hop, chunk, z).wait_send()
    for way, chunk in ((0, CO), (1, CM), (0, CR0), (1, CR1)):
        ag_copy(way, 3, chunk, z).wait_send()
    for g in range(4):
        over_peers(lambda j: ret_copy(g, j, me).wait_send())
    for n in range(NZ):
        oth_copy(n).wait_send()
    mix_drain()
    moe_drain()


def fused(*args):
    vmem = pl.BlockSpec(memory_space=pltpu.VMEM)
    hbm = pl.BlockSpec(memory_space=pl.ANY)
    sem = pltpu.SemaphoreType.DMA
    scratch = [
        pltpu.VMEM(s, t)
        for s, t in (
            ((1024, 128), BF16), ((1024, 128), BF16), ((1024, 256), BF16), ((1024, 256), BF16),
            ((NZ, BLOCK), F32), ((256, D), BF16),
            ((2, NE * PAD, 128), BF16), ((3, 2, 128, NE * RET), BF16), ((2, 128, NE * PAD), BF16),
            ((ROWS, NE * PAD), BF16), ((NE * RET, 3 * ROWS), BF16), ((4, 128, 128), F32),
            ((TM, D), BF16), ((4, TM, 128), BF16), ((1024, 128), BF16),
            ((2, D, 256), BF16), ((256, D), BF16), ((2, D, 256), BF16), ((256, D), BF16),
            ((TM, D), BF16), ((2, TM, 128), BF16),
            ((NE, PAD, D), BF16), ((NE, PAD, D), BF16),
            ((NZ, TM, D), BF16), ((NZ, 2 * TM, 128), BF16), ((NZ, 2, HALF, D), BF16),
            ((3, ROWS, 256), BF16),
            ((4, NE, RET, D), BF16), ((4, NE, RET, D), BF16),
            ((NZ, TM, D), F32), ((NZ, TM, D), BF16), ((NZ, TM, D), BF16),
            ((2, NZ, 64, D), BF16), ((NZ, 64, D), BF16),
            ((2, 4, TM, D), BF16), ((2, 4, TM, D), BF16),
            ((2, 4, 64, D), BF16), ((2, 4, 64, D), BF16),
            ((144, 256), BF16), ((NE, 144, 256), BF16),
            ((NZ, BLOCK, 256), F32), ((BLOCK, 256), F32), ((BLOCK, 256), F32),
            ((NZ, BLOCK), F32), ((NZ, BLOCK), F32),
        )
    ] + [
        sem((12,)), sem((6,)), sem((6,)), sem((6,)), sem((3,)), sem((3,)), sem((NE,)), sem((NE,)),
        sem((2, 4, 4)), sem((2, 4, 4)), sem((NE,)), sem((NE,)),
        sem((4, NE)), sem((4, NE)), sem((NZ,)), sem((NZ,)), sem, sem,
        sem((2, 4, 2)), sem((2, 4, 2)), sem((2, 4, 2)), sem((2, 4, 2)),
    ]
    return pl.pallas_call(
        kernel,
        out_shape=(jax.ShapeDtypeStruct((64, D), BF16), jax.ShapeDtypeStruct((TM, D), BF16)),
        in_specs=[vmem] * 4 + [hbm] * 18,
        out_specs=(vmem, vmem),
        scratch_shapes=scratch,
        compiler_params=pltpu.CompilerParams(
            collective_id=0, has_side_effects=True, vmem_limit_bytes=67043328
        ),
    )(*args)


def local(
    query_rows, key_rows, value_rows, gate_rows, log_decay, out_weight, channel_input, norm_gain,
    routes, route_weight, expert_gate, expert_up, expert_down, shared_gate, shared_up, shared_down,
):
    return fused(
        channel_input, norm_gain.reshape(1, D), routes, route_weight,
        query_rows, key_rows, value_rows, gate_rows, log_decay.reshape(NZ, BLOCK), out_weight,
        expert_gate, expert_up, expert_down, shared_gate, shared_up, shared_down,
        *constants(),
    )


def solution(mesh):
    split = Mesh(mesh.devices.reshape(4, 4, NZ, 2), ALL)
    return jax.shard_map(
        local,
        mesh=split,
        in_specs=(
            P(EP, TP), P(EP, TP), P(EP, TP), P(EP, TP), P(TP, EP), P(TP, None),
            P(ALL, None), P(), P(ALL, None), P(ALL, None),
            P(EP, None, TP), P(EP, None, TP), P(EP, TP, None),
            P(None, TP), P(None, TP), P(TP, None),
        ),
        out_specs=(P(ALL, None), P(ALL, None)),
        check_vma=False,
    )
```

```python
import functools

import jax
import jax.numpy as jnp
import numpy as np
from jax import lax
from jax.experimental import pallas as pl
from jax.experimental.pallas import tpu as pltpu
from jax.sharding import Mesh
from jax.sharding import PartitionSpec as P

EP = ("y", "x")
TP = ("z", "c")
ALL = ("y", "x", "z", "c")
MESH = pl.DeviceIdType.MESH
F32 = jnp.float32
BF16 = jnp.bfloat16
epsilon = 1e-06
turn_base = 10000.0

D = 2048
NE = 16
NZ = 8
BLOCK = 128
CAP = 5
TM = 48
PAIR = 2 * CAP
ROWS = NE * PAIR
HALF = ROWS // 2
PAD = 16
CO, CM, CR0, CR1 = 0, 1, 2, 3
PARCELS = ((0, 0, 16), (1, 0, 16), (1, 16, 24), (2, 0, 16), (2, 16, 16))
HEIGHTS = (16, 48, 32)
BLOCKS = (
    (0, 0), (2, 2), (2, 0), (0, 2), (3, 1), (1, 3), (3, 3), (1, 1),
    (3, 2), (2, 3), (1, 2), (2, 1), (3, 0), (0, 3), (1, 0), (0, 1),
)
BACK = tuple(BLOCKS.index((-dy % 4, -dx % 4)) for dy, dx in BLOCKS)
HB = NE // 2


def dot(a, b, dims=None, precision=None):
    if dims is None:
        return jnp.dot(a, b, preferred_element_type=F32, precision=precision)
    return lax.dot_general(a, b, (dims, ((), ())), preferred_element_type=F32)


def silu(v):
    return v / (1.0 + jnp.exp(-v))


def constants():
    place = np.zeros((2, NE * PAD, 128), np.float32)
    select = np.zeros((HALF, HB * PAD), np.float32)
    near_first = np.zeros((HB * 16, 2 * HALF), np.float32)
    near_rest = np.zeros((HB * 32, 4 * HALF), np.float32)
    far_first = np.zeros((HB * 16, 2 * HALF), np.float32)
    far_rest = np.zeros((HB * 16, 3 * HALF), np.float32)
    for j in range(NE):
        for rel in range(2):
            for p in range(CAP):
                place[rel, j * PAD + rel * CAP + p, j * CAP + p] = 1
    for b in range(HB):
        for r in range(PAIR):
            select[b * PAIR + r, b * PAD + r] = 1
            for zi in range(4):
                row, column = zi * PAIR + r, zi * HALF + b * PAIR + r
                if row < 16:
                    near_first[b * 16 + row, column] = far_first[b * 16 + row, column] = 1
                else:
                    near_rest[b * 32 + row - 16, column] = 1
                    if zi < 3:
                        far_rest[b * 16 + row - 16, column] = 1
    rate = turn_base ** (-(np.arange(128) % 64) / 64.0)
    near = np.arange(BLOCK)[:, None] * rate
    far = np.arange(128)[:, None] * float(BLOCK) * rate
    turns = np.stack([np.cos(near), np.sin(near), np.cos(far), np.sin(far)])
    tables = (place, select, near_first, near_rest, far_first, far_rest)
    return [jnp.asarray(m, BF16) for m in tables] + [jnp.asarray(turns, F32)]


def kernel(
    chan_ref, gain_ref, routes_ref, share_ref,
    q_hbm, k_hbm, v_hbm, g_hbm, decay_hbm, ow_hbm,
    eg_ref, eu_ref, ed_ref, sg_ref, su_ref, sd_ref,
    cplace_hbm, cselect_hbm, near1_hbm, near2_hbm, far1_hbm, far2_hbm, turns_hbm,
    mixer_ref, channel_ref,
    q_ref, k_ref, v_ref, g_ref, decay_ref, ow_ref,
    cplace_ref, cselect_ref, near1_ref, near2_ref, far1_ref, far2_ref, turns_ref, normed_ref, meta_ref, keys,
    wr, wd, ws, wsd, pn, pm, outg, a2a, ag_o, ag_m, ag_r, near_hid, far_hid,
    ret0_s, ret1_s, ret2_s, ret0_r, ret1_r, ret2_r,
    acc, oth, othp, mix, mixp, rs_s, rs_r, rm_s, rm_r,
    st_s, st_r, before, state, entry, run_s, off_s,
    in_sem, load_sem, w_s, w_r, pair_s, pair_r, a2a_s, a2a_r, ag_s, ag_v, st_ss, st_rs,
    ret_ss, ret_rs, oth_s, oth_r, mixp_s, mixp_r, rs_ss, rs_rs, rm_ss, rm_rs,
):
    y, x, z, c = (lax.axis_index(a) for a in ALL)
    me = y * 4 + x
    pc = 1 - c
    zup, zdown = lax.rem(z + 1, NZ), lax.rem(z + NZ - 1, NZ)
    partner = {"c": pc}

    def zat(offset):
        return lax.rem(z + (offset + NZ), NZ)

    def peer(j):
        return {"y": lax.div(j, 4), "x": lax.rem(j, 4)}

    columns = [lax.rem(y + dy, 4) * 4 + lax.rem(x + dx, 4) for dy, dx in BLOCKS]

    def rcopy(src, dst, ss, rs, dev):
        return pltpu.make_async_remote_copy(
            src_ref=src, dst_ref=dst, send_sem=ss, recv_sem=rs, device_id=dev, device_id_type=MESH
        )

    ret_s, ret_r = (ret0_s, ret1_s, ret2_s), (ret0_r, ret1_r, ret2_r)
    ret1_r[:, pl.ds(32, 16), :] = jnp.zeros((NE, 16, D), BF16)
    barrier = pltpu.get_barrier_semaphore()
    for j in columns[1:]:
        pl.semaphore_signal(barrier, inc=1, device_id=peer(j), device_id_type=MESH)
    for dev in ({"z": zup}, {"z": zdown}, partner):
        pl.semaphore_signal(barrier, inc=1, device_id=dev, device_id_type=MESH)
    incoming = [
        (cplace_hbm, cplace_ref), (k_hbm, k_ref), (v_hbm, v_ref), (decay_hbm, decay_ref),
        (turns_hbm, turns_ref), (cselect_hbm, cselect_ref), (q_hbm, q_ref), (g_hbm, g_ref),
        (ow_hbm, ow_ref), (near1_hbm, near1_ref), (near2_hbm, near2_ref), (far1_hbm, far1_ref),
        (far2_hbm, far2_ref),
    ]
    arriving = [pltpu.make_async_copy(s, d, in_sem.at[n]) for n, (s, d) in enumerate(incoming)]
    for copy in arriving:
        copy.start()

    wide_rows = chan_ref[...].astype(F32)
    mean = jnp.mean(wide_rows * wide_rows, axis=-1, keepdims=True)
    normed_ref[...] = (wide_rows * lax.rsqrt(mean + epsilon) * gain_ref[...]).astype(BF16)
    lanes = lax.broadcasted_iota(jnp.int32, (TM, 128), 1).astype(F32)
    token_r = lax.broadcasted_iota(jnp.int32, (TM, TM), 0)
    token_c = lax.broadcasted_iota(jnp.int32, (TM, TM), 1)
    unit = (token_r == token_c).astype(F32)

    def upright(rows):
        flipped = lax.dot_general(
            unit, rows, (((1,), (1,)), ((), ())), precision=lax.Precision.HIGHEST,
            preferred_element_type=F32,
        )
        return [flipped[:, k : k + 1] for k in (0, 1)]

    picks = upright(routes_ref[...].astype(F32))
    gains = upright(share_ref[...])
    hits = [(lanes == pick).astype(F32) for pick in picks]
    strict = token_r > token_c
    earlier = dot(strict.astype(F32).astype(BF16), (hits[0] + hits[1]).astype(BF16))
    metas = [jnp.zeros((TM, 128), F32)] * 4
    for k in (0, 1):
        rank = jnp.sum(earlier * hits[k], axis=-1, keepdims=True)
        column = jnp.floor(picks[k] * 0.5)
        there = (lanes == column * CAP + rank).astype(F32)
        for parity in (0, 1):
            mine = there * (picks[k] - 2 * column == parity).astype(F32)
            metas[parity] += mine
            metas[2 + parity] += mine * gains[k]
    for n in range(4):
        meta_ref[n] = metas[n].astype(BF16)
    pl.semaphore_wait(barrier, NE + 2)

    pair = [
        rcopy(normed_ref, pn, pair_s.at[0], pair_r.at[0], partner),
        rcopy(meta_ref.at[pc], pm.at[0], pair_s.at[1], pair_r.at[1], partner),
        rcopy(meta_ref.at[2 + pc], pm.at[1], pair_s.at[2], pair_r.at[2], partner),
    ]
    for copy in pair:
        copy.start()

    def ag_copy(way, hop, chunk, src_z, first=False):
        buf = {CO: ag_o.at[src_z], CM: ag_m.at[src_z]}.get(chunk)
        if buf is None:
            buf = ag_r.at[src_z, chunk - CR0]
        src = normed_ref if first and chunk == CO else buf
        dev = {"z": zup if way == 0 else zdown}
        return rcopy(src, buf, ag_s.at[way, hop, chunk], ag_v.at[way, hop, chunk], dev)

    def ag_start(way, hop, chunk):
        ag_copy(way, hop, chunk, zat(-hop if way == 0 else hop)).start()

    def ag_wait(way, hop, chunk):
        ag_copy(way, hop, chunk, zat(-(hop + 1) if way == 0 else hop + 1)).wait_recv()

    for way in (0, 1):
        ag_copy(way, 0, CO, z, first=True).start()
    weights = [
        (eg_ref.at[pc], wr.at[1, :, pl.ds(0, 128)]),
        (eu_ref.at[pc], wr.at[1, :, pl.ds(128, 128)]),
        (ed_ref.at[pc], wd.at[pl.ds(128, 128)]),
        (sg_ref, ws.at[1, :, pl.ds(0, 128)]),
        (su_ref, ws.at[1, :, pl.ds(128, 128)]),
        (sd_ref, wsd.at[pl.ds(128, 128)]),
    ]
    sent = [rcopy(s, d, w_s.at[n], w_r.at[n], partner) for n, (s, d) in enumerate(weights)]
    loads = [
        (eg_ref.at[c], wr.at[0, :, pl.ds(0, 128)]),
        (eu_ref.at[c], wr.at[0, :, pl.ds(128, 128)]),
        (ed_ref.at[c], wd.at[pl.ds(0, 128)]),
        (sg_ref, ws.at[0, :, pl.ds(0, 128)]),
        (su_ref, ws.at[0, :, pl.ds(128, 128)]),
        (sd_ref, wsd.at[pl.ds(0, 128)]),
    ]
    loaded = [pltpu.make_async_copy(s, d, load_sem.at[n]) for n, (s, d) in enumerate(loads)]
    for copy in loaded:
        copy.start()
    ag_o[z] = normed_ref[...]
    ag_m[z, pl.ds(0, TM)] = meta_ref[2 + c]
    for copy in pair:
        copy.wait_recv()
    ag_m[z, pl.ds(TM, TM)] = pm[1]
    for way in (0, 1):
        ag_start(way, 0, CM)

    def wide(count, body):
        def step(n, carry):
            body(pl.ds(pl.multiple_of(n * (D // count), D // count), D // count))
            return carry

        lax.fori_loop(0, count, step, 0)

    arriving[0].wait()
    own_pick = dot(cplace_ref[0], meta_ref[c], ((1,), (1,))).astype(BF16)
    other_pick = dot(cplace_ref[1], pm[0], ((1,), (1,))).astype(BF16)

    def gather_rows(cols):
        rows = dot(own_pick, normed_ref[:, cols]) + dot(other_pick, pn[:, cols])
        outg[:, :, cols] = rows.astype(BF16).reshape(NE, PAD, D // 4)

    wide(4, gather_rows)

    def a2a_copy(r, slot):
        return rcopy(
            outg.at[columns[r]], a2a.at[slot], a2a_s.at[r], a2a_r.at[slot], peer(columns[r])
        )

    for r in range(1, NE):
        a2a_copy(r, BACK[r]).start()
    a2a[0] = outg[me]

    def relay_own(hop):
        for chunk in (CO, CM):
            for way in (0, 1):
                ag_wait(way, hop, chunk)
        if hop < 2:
            for chunk in (CO, CM):
                for way in (0, 1):
                    ag_start(way, hop + 1, chunk)
        else:
            ag_start(0, 3, CO)
            ag_start(1, 3, CM)

    for copy in arriving[1:5]:
        copy.wait()
    half_lane = lax.broadcasted_iota(jnp.int32, (BLOCK, BLOCK), 1) < 64

    def turned(ref, n):
        rows = ref[pl.ds(pl.multiple_of(n * BLOCK, BLOCK), BLOCK), :].astype(F32)
        far_line = pl.ds(me * NZ + n, 1)
        near_cos, near_sin = turns_ref[0], turns_ref[1]
        far_cos, far_sin = turns_ref[2, far_line, :], turns_ref[3, far_line, :]
        cosine = far_cos * near_cos - far_sin * near_sin
        sine = far_sin * near_cos + far_cos * near_sin
        swapped = pltpu.roll(rows, 64, 1)
        return (rows * cosine + swapped * jnp.where(half_lane, -sine, sine)).astype(BF16)

    rows_i = lax.broadcasted_iota(jnp.int32, (BLOCK, BLOCK), 0)
    cols_i = lax.broadcasted_iota(jnp.int32, (BLOCK, BLOCK), 1)
    upper = (rows_i <= cols_i).astype(F32)
    lower = rows_i >= cols_i
    run_s[...] = dot(decay_ref[...], upper, precision=lax.Precision.HIGHEST)
    state[...] = jnp.zeros_like(state)

    def along(row):
        return jnp.transpose(jnp.broadcast_to(row, (BLOCK, BLOCK)))

    def local_state(n, total):
        rows = pl.ds(pl.multiple_of(n * BLOCK, BLOCK), BLOCK)
        row = run_s[pl.ds(n, 1), :]
        end = row[:, BLOCK - 1 :]
        off_s[pl.ds(n, 1), :] = jnp.broadcast_to(total, (1, BLOCK))
        tail = jnp.exp(end - along(row))
        key = turned(k_ref, n)
        keys[rows, :] = key
        keyed = (key.astype(F32) * tail).astype(BF16)
        before[n] = state[...]
        state[...] = jnp.exp(end) * state[...] + dot(keyed, v_ref[rows, :], ((0,), (0,)))
        return total + end

    total = lax.fori_loop(0, NZ, local_state, jnp.zeros((1, 1), F32))
    st_s[pl.ds(0, BLOCK), :] = state[...].astype(BF16)
    high = total.astype(BF16).astype(F32)
    middle = (total - high).astype(BF16).astype(F32)
    low = total - high - middle
    line = lax.broadcasted_iota(jnp.int32, (16, 256), 0)
    pieces = jnp.where(line == 0, high, jnp.where(line == 1, middle, jnp.where(line == 2, low, 0.0)))
    st_s[pl.ds(BLOCK, 16), :] = pieces.astype(BF16)

    def st_copy(j, slot):
        return rcopy(st_s, st_r.at[slot], st_ss.at[j], st_rs.at[slot], peer(j))

    def each_later(body):
        for j in columns[1:]:

            @pl.when(j > me)
            def _():
                body(j)

    relay_own(0)
    for copy in sent:
        copy.start()

    arriving[5].wait()
    for k in (0, 1):
        for r in range(max(1, k * HB), (k + 1) * HB):
            a2a_copy(r, r).wait_recv()
        if k == 1:
            each_later(lambda j: st_copy(j, me).start())

        def pack_rows(cols):
            rows = dot(cselect_ref[...], a2a[pl.ds(k * HB, HB), :, cols].reshape(HB * PAD, D // 4))
            ag_r[z, k, :, cols] = rows.astype(BF16)

        wide(4, pack_rows)
        for way in (0, 1):
            ag_start(way, 0, CR0 + k)
        if k == 0:
            relay_own(1)
    for copy in loaded + arriving[9:]:
        copy.wait()
    for copy in sent:
        copy.wait_recv()

    def hidden(rows, weight):
        parts = []
        for n in (0, 1):
            both = dot(rows, weight[n])
            parts.append((silu(both[:, :128]) * both[:, 128:]).astype(BF16))
        return jnp.concatenate(parts, axis=1)

    def shared(za, zb=None):
        rows = ag_o[za] if zb is None else jnp.concatenate([ag_o[za], ag_o[zb]], axis=0)
        h = hidden(rows, ws)

        def down(cols):
            result = dot(h, wsd[:, cols])
            acc[za, :, cols] = result[:TM]
            if zb is not None:
                acc[zb, :, cols] = result[TM:]

        wide(4, down)

    def ret_copy(n, r, slot):
        buffer, first, count = PARCELS[n]
        rows = pl.ds(first, count)
        return rcopy(
            ret_s[buffer].at[r, rows], ret_r[buffer].at[slot, rows], ret_ss.at[n, r],
            ret_rs.at[n, slot], peer(columns[r]),
        )

    def give_back(n, first, count, placed):
        buffer, top, _ = PARCELS[n]
        height = placed.shape[0] // count

        def down(cols):
            result = dot(placed, wd[:, cols]).astype(BF16)
            ret_s[buffer][pl.ds(first, count), pl.ds(top, height), cols] = result.reshape(
                count, height, D // 8
            )

        wide(8, down)
        for r in range(max(first, 1), first + count):
            ret_copy(n, r, me).start()
        if first == 0:
            rows = pl.ds(top, height)
            ret_r[buffer][me, rows] = ret_s[buffer][0, rows]

    own_hidden = hidden(ag_r[z].reshape(ROWS, D), wr)
    own_placed = [
        dot(cselect_ref[...], own_hidden[k * HALF : (k + 1) * HALF], ((0,), (0,))).astype(BF16)
        for k in (0, 1)
    ]
    give_back(0, 0, NE, jnp.concatenate(own_placed, axis=0))
    shared(z)

    entry[...] = jnp.zeros_like(entry)

    def take_state(j, carry):
        @pl.when(j < me)
        def _():
            st_copy(j, j).wait_recv()
            sums = st_r[j, pl.ds(BLOCK, 16), :].astype(F32)
            decay = jnp.exp(sums[0:1] + sums[1:2] + sums[2:3])
            entry[...] = decay * entry[...] + st_r[j, pl.ds(0, BLOCK), :].astype(F32)

        return carry


    def retain(n, carry):
        rows = pl.ds(pl.multiple_of(n * BLOCK, BLOCK), BLOCK)
        row = run_s[pl.ds(n, 1), :]
        spread = along(row)
        query, key, value = turned(q_ref, n), keys[rows, :], v_ref[rows, :]
        scores = dot(query, key, ((1,), (1,)))
        factor = jnp.exp(jnp.where(lower, spread - row, 0.0))
        mixed = jnp.where(lower, scores * factor, 0.0).astype(BF16)
        scaled_query = (query.astype(F32) * jnp.exp(spread)).astype(BF16)
        offset = jnp.exp(off_s[pl.ds(n, 1), :][:, 0:1])
        prior = (before[n] + offset * entry[...]).astype(BF16)
        kept = dot(mixed, value) + dot(scaled_query, prior)
        scale = lax.rsqrt(jnp.mean(kept * kept, axis=-1, keepdims=True) + epsilon)
        gated = (silu(g_ref[rows, :].astype(F32)) * (kept * scale)).astype(BF16)

        def project(cols):
            term = dot(gated, ow_ref[:, cols]).astype(BF16)
            mix[0, n, :, cols] = term[:64]
            mix[1, n, :, cols] = term[64:]

        wide(4, project)
        return carry

    mix_copy = rcopy(mix.at[pc], mixp, mixp_s, mixp_r, partner)

    def retain_two(n):
        lax.fori_loop(2 * n, 2 * n + 2, retain, 0)

    for h in (1, 2, 3):
        za, zb = zat(-h), zat(h)
        for k in (0, 1):
            for way in (0, 1):
                ag_wait(way, h - 1, CR0 + k)
            for way in (0, 1):
                if h < 3 or way == k:
                    ag_start(way, h, CR0 + k)
            h_rows = hidden(jnp.concatenate([ag_r[za, k], ag_r[zb, k]], axis=0), wr)
            if h == 1:
                near_hid[k, pl.ds(0, 2 * HALF)] = h_rows
                give_back(1, k * HB, HB, dot(near1_ref[...], h_rows).astype(BF16))
            elif h == 2:
                near_hid[k, pl.ds(2 * HALF, 2 * HALF)] = h_rows
                give_back(2, k * HB, HB, dot(near2_ref[...], near_hid[k]).astype(BF16))
            else:
                far_hid[k, pl.ds(0, 2 * HALF)] = h_rows
                give_back(3, k * HB, HB, dot(far1_ref[...], h_rows).astype(BF16))
            if (h, k) == (1, 0):
                relay_own(2)
            if (h, k) == (1, 1):
                for copy in arriving[6:9]:
                    copy.wait()
                lax.fori_loop(0, NE - 1, take_state, 0)
                retain_two(0)
            elif (h, k) == (2, 0):
                retain_two(1)
            elif (h, k) == (2, 1):
                retain_two(2)
            elif (h, k) == (3, 0):
                retain_two(3)
                mix_copy.start()
        if h < 3:
            shared(za, zb)
    def chain(base, send, recv, ss, rs):
        width = D // 4

        def copy(way, s, part):
            dev = {"z": zup if way == 0 else zdown}
            cols = pl.ds(part * width, width)
            return rcopy(
                send.at[way, s, :, cols], recv.at[way, s, :, cols], ss.at[way, s, part],
                rs.at[way, s, part], dev,
            )

        def forward(s, part):
            for way in (0, 1):
                hop = s if part // 2 == way else s + 1
                if hop > 3:
                    continue
                target = zat(4 - hop if way == 0 else hop - 4)
                cols = pl.ds(part * width, width)
                value = base(target, cols)
                if s > 0:
                    copy(way, hop - 1, part).wait_recv()
                    value = value + recv[way, hop - 1, :, cols].astype(F32)
                send[way, hop, :, cols] = value.astype(BF16)
                copy(way, hop, part).start()

        def step(s):
            for part in (0, 2, 1, 3):
                forward(s, part)

        def finish(out_ref):
            for part in (0, 2, 1, 3):
                cols = pl.ds(part * width, width)
                value = base(z, cols)
                for way in (0, 1):
                    copy(way, 3, part).wait_recv()
                    value = value + recv[way, 3, :, cols].astype(F32)
                out_ref[:, cols] = value.astype(BF16)

        def drain():
            for way in (0, 1):
                for s in range(4):
                    for part in range(4):
                        if s or part // 2 == way:
                            copy(way, s, part).wait_send()

        return step, finish, drain

    def mix_base(target, cols):
        return mix[c, target, :, cols].astype(F32) + mixp[target, :, cols].astype(F32)

    def moe_base(target, cols):
        return acc[target, :, cols] + othp[target, :, cols].astype(F32)

    mix_step, mix_finish, mix_drain = chain(mix_base, rm_s, rm_r, rm_ss, rm_rs)
    moe_step, moe_finish, moe_drain = chain(moe_base, rs_s, rs_r, rs_ss, rs_rs)

    sources = [(0, 0, 0), (1, 0, -1), (1, 1, 1), (1, 2, -2), (1, 3, 2), (2, 0, -3), (2, 1, 3), (2, 2, 4)]

    def oth_copy(n):
        where = zat(sources[n][2])
        return rcopy(oth.at[where], othp.at[where], oth_s.at[n], oth_r.at[n], partner)

    def combine(buffer):
        for n in range(5):
            if PARCELS[n][0] == buffer:
                for r in range(1, NE):
                    ret_copy(n, r, columns[r]).wait_recv()
        height = HEIGHTS[buffer]
        lane = lax.broadcasted_iota(jnp.int32, (128, NE * height), 0).astype(F32)
        place = lax.broadcasted_iota(jnp.int32, (128, NE * height), 1).astype(F32)
        column = jnp.floor((lane + 0.5) * (1.0 / CAP))
        ahead = place - (column * height + (lane - column * CAP))
        group = [(n, zi, zat(offset)) for n, (at, zi, offset) in enumerate(sources) if at == buffer]
        spread = []
        for n, zi, where in group:
            weight = ag_m[where]
            for rel in (0, 1):
                table = (ahead == zi * PAIR + rel * CAP).astype(F32).astype(BF16)
                spread.append(dot(weight[rel * TM : (rel + 1) * TM], table))
        spread = jnp.concatenate(spread, axis=0).astype(BF16)

        def gather(cols):
            rows = ret_r[buffer][:, :, cols].reshape(NE * height, D // 4)
            result = dot(spread, rows)
            for at, (n, zi, where) in enumerate(group):
                acc[where, :, cols] += result[2 * at * TM : (2 * at + 1) * TM]
                oth[where, :, cols] = result[(2 * at + 1) * TM : (2 * at + 2) * TM].astype(BF16)

        wide(4, gather)
        for n, zi, where in group:
            oth_copy(n).start()

    mix_copy.wait_recv()
    mix_step(0)
    opposite = zat(4)
    for k in (0, 1):
        ag_wait(k, 3, CR0 + k)
        far_hid[k, pl.ds(2 * HALF, HALF)] = hidden(ag_r[opposite, k], wr)
        give_back(4, k * HB, HB, dot(far2_ref[...], far_hid[k]).astype(BF16))
    shared(zat(-3), zat(3))
    mix_step(1)
    ag_wait(0, 3, CO)
    ag_wait(1, 3, CM)
    shared(opposite)
    combine(0)
    mix_step(2)
    combine(1)
    mix_step(3)
    combine(2)
    for n in range(NZ):
        oth_copy(n).wait_recv()
    moe_step(0)
    mix_finish(mixer_ref)
    for s in (1, 2, 3):
        moe_step(s)
    moe_finish(channel_ref)

    for copy in pair + sent + [mix_copy]:
        copy.wait_send()
    for r in range(1, NE):
        a2a_copy(r, r).wait_send()
    each_later(lambda j: st_copy(j, me).wait_send())
    for way in (0, 1):
        ag_copy(way, 0, CO, z, first=True).wait_send()
        for hop in range(3):
            for chunk in (CO, CM, CR0, CR1):
                if hop or chunk != CO:
                    ag_copy(way, hop, chunk, z).wait_send()
    for way, chunk in ((0, CO), (1, CM), (0, CR0), (1, CR1)):
        ag_copy(way, 3, chunk, z).wait_send()
    for g in range(5):
        for r in range(1, NE):
            ret_copy(g, r, me).wait_send()
    for n in range(NZ):
        oth_copy(n).wait_send()
    mix_drain()
    moe_drain()


def fused(*args):
    vmem = pl.BlockSpec(memory_space=pltpu.VMEM)
    hbm = pl.BlockSpec(memory_space=pl.ANY)
    sem = pltpu.SemaphoreType.DMA
    scratch = [
        pltpu.VMEM(s, t)
        for s, t in (
            ((1024, 128), BF16), ((1024, 128), BF16), ((1024, 256), BF16), ((1024, 256), BF16),
            ((NZ, BLOCK), F32), ((256, D), BF16),
            ((2, NE * PAD, 128), BF16), ((HALF, HB * PAD), BF16),
            ((HB * 16, 2 * HALF), BF16), ((HB * 32, 4 * HALF), BF16), ((HB * 16, 2 * HALF), BF16),
            ((HB * 16, 3 * HALF), BF16), ((4, 128, 128), F32),
            ((TM, D), BF16), ((4, TM, 128), BF16), ((1024, 128), BF16),
            ((2, D, 256), BF16), ((256, D), BF16), ((2, D, 256), BF16), ((256, D), BF16),
            ((TM, D), BF16), ((2, TM, 128), BF16),
            ((NE, PAD, D), BF16), ((NE, PAD, D), BF16),
            ((NZ, TM, D), BF16), ((NZ, 2 * TM, 128), BF16), ((NZ, 2, HALF, D), BF16),
            ((2, 4 * HALF, 256), BF16), ((2, 3 * HALF, 256), BF16),
            *(((NE, n, D), BF16) for n in HEIGHTS + HEIGHTS),
            ((NZ, TM, D), F32), ((NZ, TM, D), BF16), ((NZ, TM, D), BF16),
            ((2, NZ, 64, D), BF16), ((NZ, 64, D), BF16),
            ((2, 4, TM, D), BF16), ((2, 4, TM, D), BF16),
            ((2, 4, 64, D), BF16), ((2, 4, 64, D), BF16),
            ((144, 256), BF16), ((NE, 144, 256), BF16),
            ((NZ, BLOCK, 256), F32), ((BLOCK, 256), F32), ((BLOCK, 256), F32),
            ((NZ, BLOCK), F32), ((NZ, BLOCK), F32),
        )
    ] + [
        sem((13,)), sem((6,)), sem((6,)), sem((6,)), sem((3,)), sem((3,)), sem((NE,)), sem((NE,)),
        sem((2, 4, 4)), sem((2, 4, 4)), sem((NE,)), sem((NE,)),
        sem((5, NE)), sem((5, NE)), sem((NZ,)), sem((NZ,)), sem, sem,
        sem((2, 4, 4)), sem((2, 4, 4)), sem((2, 4, 4)), sem((2, 4, 4)),
    ]
    return pl.pallas_call(
        kernel,
        out_shape=(jax.ShapeDtypeStruct((64, D), BF16), jax.ShapeDtypeStruct((TM, D), BF16)),
        in_specs=[vmem] * 4 + [hbm] * 19,
        out_specs=(vmem, vmem),
        scratch_shapes=scratch,
        compiler_params=pltpu.CompilerParams(
            collective_id=0, has_side_effects=True, vmem_limit_bytes=67043328
        ),
    )(*args)


def local(
    query_rows, key_rows, value_rows, gate_rows, log_decay, out_weight, channel_input, norm_gain,
    routes, route_weight, expert_gate, expert_up, expert_down, shared_gate, shared_up, shared_down,
):
    return fused(
        channel_input, norm_gain.reshape(1, D), routes.T, route_weight.T,
        query_rows, key_rows, value_rows, gate_rows, log_decay.reshape(NZ, BLOCK), out_weight,
        expert_gate, expert_up, expert_down, shared_gate, shared_up, shared_down,
        *constants(),
    )


def solution(mesh):
    split = Mesh(mesh.devices.reshape(4, 4, NZ, 2), ALL)
    return jax.shard_map(
        local,
        mesh=split,
        in_specs=(
            P(EP, TP), P(EP, TP), P(EP, TP), P(EP, TP), P(TP, EP), P(TP, None),
            P(ALL, None), P(), P(ALL, None), P(ALL, None),
            P(EP, None, TP), P(EP, None, TP), P(EP, TP, None),
            P(None, TP), P(None, TP), P(TP, None),
        ),
        out_specs=(P(ALL, None), P(ALL, None)),
        check_vma=False,
    )
```

```python
import functools

import jax
import jax.numpy as jnp
import numpy as np
from jax import lax
from jax.experimental import pallas as pl
from jax.experimental.pallas import tpu as pltpu
from jax.sharding import Mesh
from jax.sharding import PartitionSpec as P

EP = ("y", "x")
TP = ("z", "c")
ALL = ("y", "x", "z", "c")
MESH = pl.DeviceIdType.MESH
F32 = jnp.float32
BF16 = jnp.bfloat16
epsilon = 1e-06
turn_base = 10000.0

D = 2048
NE = 16
NZ = 8
BLOCK = 128
CAP = 5
TM = 48
PAIR = 2 * CAP
ROWS = NE * PAIR
HALF = ROWS // 2
PAD = 16
CO, CM, CR0, CR1 = 0, 1, 2, 3
PARCELS = ((0, 0, 16), (1, 0, 16), (1, 16, 24), (2, 0, 16), (2, 16, 16))
HEIGHTS = (16, 48, 32)
BLOCKS = (
    (0, 0), (2, 2), (0, 2), (2, 0), (1, 3), (3, 1), (3, 3), (1, 1),
    (2, 3), (3, 2), (2, 1), (1, 2), (0, 3), (3, 0), (0, 1), (1, 0),
)
BACK = tuple(BLOCKS.index((-dy % 4, -dx % 4)) for dy, dx in BLOCKS)
HB = NE // 2


def dot(a, b, dims=None, precision=None):
    if dims is None:
        return jnp.dot(a, b, preferred_element_type=F32, precision=precision)
    return lax.dot_general(a, b, (dims, ((), ())), preferred_element_type=F32)


def silu(v):
    return v / (1.0 + jnp.exp(-v))


def constants():
    place = np.zeros((2, NE * PAD, 128), np.float32)
    select = np.zeros((HALF, HB * PAD), np.float32)
    near_first = np.zeros((HB * 16, 2 * HALF), np.float32)
    near_rest = np.zeros((HB * 32, 4 * HALF), np.float32)
    far_first = np.zeros((HB * 16, 2 * HALF), np.float32)
    far_rest = np.zeros((HB * 16, 3 * HALF), np.float32)
    for j in range(NE):
        for rel in range(2):
            for p in range(CAP):
                place[rel, j * PAD + rel * CAP + p, j * CAP + p] = 1
    for b in range(HB):
        for r in range(PAIR):
            select[b * PAIR + r, b * PAD + r] = 1
            for zi in range(4):
                row, column = zi * PAIR + r, zi * HALF + b * PAIR + r
                if row < 16:
                    near_first[b * 16 + row, column] = far_first[b * 16 + row, column] = 1
                else:
                    near_rest[b * 32 + row - 16, column] = 1
                    if zi < 3:
                        far_rest[b * 16 + row - 16, column] = 1
    rate = turn_base ** (-(np.arange(128) % 64) / 64.0)
    near = np.arange(BLOCK)[:, None] * rate
    far = np.arange(128)[:, None] * float(BLOCK) * rate
    turns = np.stack([np.cos(near), np.sin(near), np.cos(far), np.sin(far)])
    tables = (place, select, near_first, near_rest, far_first, far_rest)
    return [jnp.asarray(m, BF16) for m in tables] + [jnp.asarray(turns, F32)]


def kernel(
    chan_hbm, gain_hbm, routes_hbm, share_hbm,
    q_hbm, k_hbm, v_hbm, g_hbm, decay_hbm, ow_hbm,
    eg_ref, eu_ref, ed_ref, sg_ref, su_ref, sd_ref,
    cplace_hbm, cselect_hbm, near1_hbm, near2_hbm, far1_hbm, far2_hbm, turns_hbm,
    mixer_ref, channel_ref,
    chan_ref, gain_ref, routes_ref, share_ref, first_sem,
    q_ref, k_ref, v_ref, g_ref, decay_ref, ow_ref,
    cplace_ref, cselect_ref, near1_ref, near2_ref, far1_ref, far2_ref, turns_ref, normed_ref, meta_ref, keys,
    wr, wd, ws, wsd, pn, pm, outg, a2a, ag_o, ag_m, ag_r, near_hid, far_hid,
    ret0_s, ret1_s, ret2_s, ret0_r, ret1_r, ret2_r,
    acc, oth, othp, mix, mixp, rs_s, rs_r, rm_s, rm_r,
    st_s, st_r, before, state, entry, run_s, off_s,
    in_sem, load_sem, w_s, w_r, pair_s, pair_r, a2a_s, a2a_r, ag_s, ag_v, st_ss, st_rs,
    ret_ss, ret_rs, oth_s, oth_r, mixp_s, mixp_r, rs_ss, rs_rs, rm_ss, rm_rs,
):
    y, x, z, c = (lax.axis_index(a) for a in ALL)
    me = y * 4 + x
    pc = 1 - c
    zup, zdown = lax.rem(z + 1, NZ), lax.rem(z + NZ - 1, NZ)
    partner = {"c": pc}

    def zat(offset):
        return lax.rem(z + (offset + NZ), NZ)

    def peer(j):
        return {"y": lax.div(j, 4), "x": lax.rem(j, 4)}

    columns = [lax.rem(y + dy, 4) * 4 + lax.rem(x + dx, 4) for dy, dx in BLOCKS]

    def rcopy(src, dst, ss, rs, dev):
        return pltpu.make_async_remote_copy(
            src_ref=src, dst_ref=dst, send_sem=ss, recv_sem=rs, device_id=dev, device_id_type=MESH
        )

    firsts = [
        (chan_hbm, chan_ref), (gain_hbm, gain_ref), (routes_hbm, routes_ref), (share_hbm, share_ref),
    ]
    firsts = [pltpu.make_async_copy(s, d, first_sem.at[n]) for n, (s, d) in enumerate(firsts)]
    for copy in firsts:
        copy.start()
    ret_s, ret_r = (ret0_s, ret1_s, ret2_s), (ret0_r, ret1_r, ret2_r)
    ret1_r[:, pl.ds(32, 16), :] = jnp.zeros((NE, 16, D), BF16)
    barrier = pltpu.get_barrier_semaphore()
    for j in columns[1:]:
        pl.semaphore_signal(barrier, inc=1, device_id=peer(j), device_id_type=MESH)
    for dev in ({"z": zup}, {"z": zdown}, partner):
        pl.semaphore_signal(barrier, inc=1, device_id=dev, device_id_type=MESH)
    incoming = [
        (cplace_hbm, cplace_ref), (k_hbm, k_ref), (v_hbm, v_ref), (decay_hbm, decay_ref),
        (turns_hbm, turns_ref), (cselect_hbm, cselect_ref), (q_hbm, q_ref), (g_hbm, g_ref),
        (ow_hbm, ow_ref), (near1_hbm, near1_ref), (near2_hbm, near2_ref), (far1_hbm, far1_ref),
        (far2_hbm, far2_ref),
    ]
    arriving = [pltpu.make_async_copy(s, d, in_sem.at[n]) for n, (s, d) in enumerate(incoming)]
    for copy in arriving:
        copy.start()

    for copy in firsts:
        copy.wait()
    wide_rows = chan_ref[...].astype(F32)
    mean = jnp.mean(wide_rows * wide_rows, axis=-1, keepdims=True)
    normed_ref[...] = (wide_rows * lax.rsqrt(mean + epsilon) * gain_ref[...]).astype(BF16)
    lanes = lax.broadcasted_iota(jnp.int32, (TM, 128), 1).astype(F32)
    token_r = lax.broadcasted_iota(jnp.int32, (TM, TM), 0)
    token_c = lax.broadcasted_iota(jnp.int32, (TM, TM), 1)
    unit = (token_r == token_c).astype(F32)

    def upright(rows):
        flipped = lax.dot_general(
            unit, rows, (((1,), (1,)), ((), ())), precision=lax.Precision.HIGHEST,
            preferred_element_type=F32,
        )
        return [flipped[:, k : k + 1] for k in (0, 1)]

    picks = upright(routes_ref[...].astype(F32))
    gains = upright(share_ref[...])
    hits = [(lanes == pick).astype(F32) for pick in picks]
    strict = token_r > token_c
    earlier = dot(strict.astype(F32).astype(BF16), (hits[0] + hits[1]).astype(BF16))
    metas = [jnp.zeros((TM, 128), F32)] * 4
    for k in (0, 1):
        rank = jnp.sum(earlier * hits[k], axis=-1, keepdims=True)
        column = jnp.floor(picks[k] * 0.5)
        there = (lanes == column * CAP + rank).astype(F32)
        for parity in (0, 1):
            mine = there * (picks[k] - 2 * column == parity).astype(F32)
            metas[parity] += mine
            metas[2 + parity] += mine * gains[k]
    for n in range(4):
        meta_ref[n] = metas[n].astype(BF16)
    pl.semaphore_wait(barrier, NE + 2)

    pair = [
        rcopy(normed_ref, pn, pair_s.at[0], pair_r.at[0], partner),
        rcopy(meta_ref.at[pc], pm.at[0], pair_s.at[1], pair_r.at[1], partner),
        rcopy(meta_ref.at[2 + pc], pm.at[1], pair_s.at[2], pair_r.at[2], partner),
    ]
    for copy in pair:
        copy.start()

    def ag_copy(way, hop, chunk, src_z, first=False):
        buf = {CO: ag_o.at[src_z], CM: ag_m.at[src_z]}.get(chunk)
        if buf is None:
            buf = ag_r.at[src_z, chunk - CR0]
        src = normed_ref if first and chunk == CO else buf
        dev = {"z": zup if way == 0 else zdown}
        return rcopy(src, buf, ag_s.at[way, hop, chunk], ag_v.at[way, hop, chunk], dev)

    def ag_start(way, hop, chunk):
        ag_copy(way, hop, chunk, zat(-hop if way == 0 else hop)).start()

    def ag_wait(way, hop, chunk):
        ag_copy(way, hop, chunk, zat(-(hop + 1) if way == 0 else hop + 1)).wait_recv()

    for way in (0, 1):
        ag_copy(way, 0, CO, z, first=True).start()
    weights = [
        (eg_ref.at[pc], wr.at[1, :, pl.ds(0, 128)]),
        (eu_ref.at[pc], wr.at[1, :, pl.ds(128, 128)]),
        (ed_ref.at[pc], wd.at[pl.ds(128, 128)]),
        (sg_ref, ws.at[1, :, pl.ds(0, 128)]),
        (su_ref, ws.at[1, :, pl.ds(128, 128)]),
        (sd_ref, wsd.at[pl.ds(128, 128)]),
    ]
    sent = [rcopy(s, d, w_s.at[n], w_r.at[n], partner) for n, (s, d) in enumerate(weights)]
    loads = [
        (eg_ref.at[c], wr.at[0, :, pl.ds(0, 128)]),
        (eu_ref.at[c], wr.at[0, :, pl.ds(128, 128)]),
        (ed_ref.at[c], wd.at[pl.ds(0, 128)]),
        (sg_ref, ws.at[0, :, pl.ds(0, 128)]),
        (su_ref, ws.at[0, :, pl.ds(128, 128)]),
        (sd_ref, wsd.at[pl.ds(0, 128)]),
    ]
    loaded = [pltpu.make_async_copy(s, d, load_sem.at[n]) for n, (s, d) in enumerate(loads)]
    for copy in loaded:
        copy.start()
    ag_o[z] = normed_ref[...]
    ag_m[z, pl.ds(0, TM)] = meta_ref[2 + c]
    for copy in pair:
        copy.wait_recv()
    ag_m[z, pl.ds(TM, TM)] = pm[1]
    for way in (0, 1):
        ag_start(way, 0, CM)

    def wide(count, body):
        def step(n, carry):
            body(pl.ds(pl.multiple_of(n * (D // count), D // count), D // count))
            return carry

        lax.fori_loop(0, count, step, 0)

    arriving[0].wait()
    own_pick = dot(cplace_ref[0], meta_ref[c], ((1,), (1,))).astype(BF16)
    other_pick = dot(cplace_ref[1], pm[0], ((1,), (1,))).astype(BF16)

    def gather_rows(cols):
        rows = dot(own_pick, normed_ref[:, cols]) + dot(other_pick, pn[:, cols])
        outg[:, :, cols] = rows.astype(BF16).reshape(NE, PAD, D // 4)

    wide(4, gather_rows)

    def a2a_copy(r, slot):
        return rcopy(
            outg.at[columns[r]], a2a.at[slot], a2a_s.at[r], a2a_r.at[slot], peer(columns[r])
        )

    for r in range(1, NE):
        a2a_copy(r, BACK[r]).start()
    a2a[0] = outg[me]

    def relay_own(hop):
        for chunk in (CO, CM):
            for way in (0, 1):
                ag_wait(way, hop, chunk)
        if hop < 2:
            for chunk in (CO, CM):
                for way in (0, 1):
                    ag_start(way, hop + 1, chunk)
        else:
            ag_start(0, 3, CO)
            ag_start(1, 3, CM)

    for copy in arriving[1:5]:
        copy.wait()
    half_lane = lax.broadcasted_iota(jnp.int32, (BLOCK, BLOCK), 1) < 64

    def turned(ref, n):
        rows = ref[pl.ds(pl.multiple_of(n * BLOCK, BLOCK), BLOCK), :].astype(F32)
        far_line = pl.ds(me * NZ + n, 1)
        near_cos, near_sin = turns_ref[0], turns_ref[1]
        far_cos, far_sin = turns_ref[2, far_line, :], turns_ref[3, far_line, :]
        cosine = far_cos * near_cos - far_sin * near_sin
        sine = far_sin * near_cos + far_cos * near_sin
        swapped = pltpu.roll(rows, 64, 1)
        return (rows * cosine + swapped * jnp.where(half_lane, -sine, sine)).astype(BF16)

    rows_i = lax.broadcasted_iota(jnp.int32, (BLOCK, BLOCK), 0)
    cols_i = lax.broadcasted_iota(jnp.int32, (BLOCK, BLOCK), 1)
    upper = (rows_i <= cols_i).astype(F32)
    lower = rows_i >= cols_i
    run_s[...] = dot(decay_ref[...], upper, precision=lax.Precision.HIGHEST)
    state[...] = jnp.zeros_like(state)

    def along(row):
        return jnp.transpose(jnp.broadcast_to(row, (BLOCK, BLOCK)))

    def local_state(n, total):
        rows = pl.ds(pl.multiple_of(n * BLOCK, BLOCK), BLOCK)
        row = run_s[pl.ds(n, 1), :]
        end = row[:, BLOCK - 1 :]
        off_s[pl.ds(n, 1), :] = jnp.broadcast_to(total, (1, BLOCK))
        tail = jnp.exp(end - along(row))
        key = turned(k_ref, n)
        keys[rows, :] = key
        keyed = (key.astype(F32) * tail).astype(BF16)
        before[n] = state[...]
        state[...] = jnp.exp(end) * state[...] + dot(keyed, v_ref[rows, :], ((0,), (0,)))
        return total + end

    total = lax.fori_loop(0, NZ, local_state, jnp.zeros((1, 1), F32))
    st_s[pl.ds(0, BLOCK), :] = state[...].astype(BF16)
    high = total.astype(BF16).astype(F32)
    middle = (total - high).astype(BF16).astype(F32)
    low = total - high - middle
    line = lax.broadcasted_iota(jnp.int32, (16, 256), 0)
    pieces = jnp.where(line == 0, high, jnp.where(line == 1, middle, jnp.where(line == 2, low, 0.0)))
    st_s[pl.ds(BLOCK, 16), :] = pieces.astype(BF16)

    def st_copy(j, slot):
        return rcopy(st_s, st_r.at[slot], st_ss.at[j], st_rs.at[slot], peer(j))

    def each_later(body):
        for j in columns[1:]:

            @pl.when(j > me)
            def _():
                body(j)

    relay_own(0)
    for copy in sent:
        copy.start()

    arriving[5].wait()
    for k in (0, 1):
        for r in range(max(1, k * HB), (k + 1) * HB):
            a2a_copy(r, r).wait_recv()
        if k == 0:
            each_later(lambda j: st_copy(j, me).start())

        def pack_rows(cols):
            rows = dot(cselect_ref[...], a2a[pl.ds(k * HB, HB), :, cols].reshape(HB * PAD, D // 4))
            ag_r[z, k, :, cols] = rows.astype(BF16)

        wide(4, pack_rows)
        for way in (0, 1):
            ag_start(way, 0, CR0 + k)
        if k == 0:
            relay_own(1)
    for copy in loaded + arriving[9:]:
        copy.wait()
    for copy in sent:
        copy.wait_recv()

    def hidden(rows, weight):
        parts = []
        for n in (0, 1):
            both = dot(rows, weight[n])
            parts.append((silu(both[:, :128]) * both[:, 128:]).astype(BF16))
        return jnp.concatenate(parts, axis=1)

    def shared(za, zb=None):
        rows = ag_o[za] if zb is None else jnp.concatenate([ag_o[za], ag_o[zb]], axis=0)
        h = hidden(rows, ws)

        def down(cols):
            result = dot(h, wsd[:, cols])
            acc[za, :, cols] = result[:TM]
            if zb is not None:
                acc[zb, :, cols] = result[TM:]

        wide(4, down)

    def ret_copy(n, r, slot):
        buffer, first, count = PARCELS[n]
        rows = pl.ds(first, count)
        return rcopy(
            ret_s[buffer].at[r, rows], ret_r[buffer].at[slot, rows], ret_ss.at[n, r],
            ret_rs.at[n, slot], peer(columns[r]),
        )

    def give_back(n, first, count, placed):
        buffer, top, _ = PARCELS[n]
        height = placed.shape[0] // count

        def down(cols):
            result = dot(placed, wd[:, cols]).astype(BF16)
            ret_s[buffer][pl.ds(first, count), pl.ds(top, height), cols] = result.reshape(
                count, height, D // 4
            )

        wide(4, down)
        for r in range(max(first, 1), first + count):
            ret_copy(n, r, me).start()
        if first == 0:
            rows = pl.ds(top, height)
            ret_r[buffer][me, rows] = ret_s[buffer][0, rows]

    own_hidden = hidden(ag_r[z].reshape(ROWS, D), wr)
    own_placed = [
        dot(cselect_ref[...], own_hidden[k * HALF : (k + 1) * HALF], ((0,), (0,))).astype(BF16)
        for k in (0, 1)
    ]
    give_back(0, 0, NE, jnp.concatenate(own_placed, axis=0))
    shared(z)

    entry[...] = jnp.zeros_like(entry)

    def take_state(j, carry):
        @pl.when(j < me)
        def _():
            st_copy(j, j).wait_recv()
            sums = st_r[j, pl.ds(BLOCK, 16), :].astype(F32)
            decay = jnp.exp(sums[0:1] + sums[1:2] + sums[2:3])
            entry[...] = decay * entry[...] + st_r[j, pl.ds(0, BLOCK), :].astype(F32)

        return carry


    def retain(n, carry):
        rows = pl.ds(pl.multiple_of(n * BLOCK, BLOCK), BLOCK)
        row = run_s[pl.ds(n, 1), :]
        spread = along(row)
        query, key, value = turned(q_ref, n), keys[rows, :], v_ref[rows, :]
        scores = dot(query, key, ((1,), (1,)))
        factor = jnp.exp(jnp.where(lower, spread - row, 0.0))
        mixed = jnp.where(lower, scores * factor, 0.0).astype(BF16)
        scaled_query = (query.astype(F32) * jnp.exp(spread)).astype(BF16)
        offset = jnp.exp(off_s[pl.ds(n, 1), :][:, 0:1])
        prior = (before[n] + offset * entry[...]).astype(BF16)
        kept = dot(mixed, value) + dot(scaled_query, prior)
        scale = lax.rsqrt(jnp.mean(kept * kept, axis=-1, keepdims=True) + epsilon)
        gated = (silu(g_ref[rows, :].astype(F32)) * (kept * scale)).astype(BF16)

        def project(cols):
            term = dot(gated, ow_ref[:, cols]).astype(BF16)
            mix[0, n, :, cols] = term[:64]
            mix[1, n, :, cols] = term[64:]

        wide(4, project)
        return carry

    mix_copy = rcopy(mix.at[pc], mixp, mixp_s, mixp_r, partner)

    def retain_some(first, last):
        lax.fori_loop(first, last, retain, 0)

    for h in (1, 2, 3):
        za, zb = zat(-h), zat(h)
        for k in (0, 1):
            for way in (0, 1):
                ag_wait(way, h - 1, CR0 + k)
            for way in (0, 1):
                if h < 3 or way == k:
                    ag_start(way, h, CR0 + k)
            h_rows = hidden(jnp.concatenate([ag_r[za, k], ag_r[zb, k]], axis=0), wr)
            if h == 1:
                near_hid[k, pl.ds(0, 2 * HALF)] = h_rows
                give_back(1, k * HB, HB, dot(near1_ref[...], h_rows).astype(BF16))
            elif h == 2:
                near_hid[k, pl.ds(2 * HALF, 2 * HALF)] = h_rows
                give_back(2, k * HB, HB, dot(near2_ref[...], near_hid[k]).astype(BF16))
            else:
                far_hid[k, pl.ds(0, 2 * HALF)] = h_rows
                give_back(3, k * HB, HB, dot(far1_ref[...], h_rows).astype(BF16))
            if (h, k) == (1, 0):
                relay_own(2)
                shared(za, zb)
            elif (h, k) == (1, 1):
                for copy in arriving[6:9]:
                    copy.wait()
                lax.fori_loop(0, NE - 1, take_state, 0)
                retain_some(0, 1)
            elif (h, k) == (2, 0):
                retain_some(1, 5)
            elif (h, k) == (2, 1):
                shared(za, zb)
            elif (h, k) == (3, 0):
                retain_some(5, 8)
                mix_copy.start()

    def chain(base, send, recv, ss, rs):
        width = D // 4

        def copy(way, s, part):
            dev = {"z": zup if way == 0 else zdown}
            cols = pl.ds(part * width, width)
            return rcopy(
                send.at[way, s, :, cols], recv.at[way, s, :, cols], ss.at[way, s, part],
                rs.at[way, s, part], dev,
            )

        def forward(s, part):
            for way in (0, 1):
                hop = s if part // 2 == way else s + 1
                if hop > 3:
                    continue
                target = zat(4 - hop if way == 0 else hop - 4)
                cols = pl.ds(part * width, width)
                value = base(target, cols)
                if s > 0:
                    copy(way, hop - 1, part).wait_recv()
                    value = value + recv[way, hop - 1, :, cols].astype(F32)
                send[way, hop, :, cols] = value.astype(BF16)
                copy(way, hop, part).start()

        def step(s):
            for part in (0, 2, 1, 3):
                forward(s, part)

        def finish(out_ref):
            for part in (0, 2, 1, 3):
                cols = pl.ds(part * width, width)
                value = base(z, cols)
                for way in (0, 1):
                    copy(way, 3, part).wait_recv()
                    value = value + recv[way, 3, :, cols].astype(F32)
                out_ref[:, cols] = value.astype(BF16)

        def drain():
            for way in (0, 1):
                for s in range(4):
                    for part in range(4):
                        if s or part // 2 == way:
                            copy(way, s, part).wait_send()

        return step, finish, drain

    def mix_base(target, cols):
        return mix[c, target, :, cols].astype(F32) + mixp[target, :, cols].astype(F32)

    def moe_base(target, cols):
        return acc[target, :, cols] + othp[target, :, cols].astype(F32)

    mix_step, mix_finish, mix_drain = chain(mix_base, rm_s, rm_r, rm_ss, rm_rs)
    moe_step, moe_finish, moe_drain = chain(moe_base, rs_s, rs_r, rs_ss, rs_rs)

    sources = [(0, 0, 0), (1, 0, -1), (1, 1, 1), (1, 2, -2), (1, 3, 2), (2, 0, -3), (2, 1, 3), (2, 2, 4)]

    def oth_copy(n):
        where = zat(sources[n][2])
        return rcopy(oth.at[where], othp.at[where], oth_s.at[n], oth_r.at[n], partner)

    def combine(buffer):
        height = HEIGHTS[buffer]
        lane = lax.broadcasted_iota(jnp.int32, (128, NE * height), 0).astype(F32)
        place = lax.broadcasted_iota(jnp.int32, (128, NE * height), 1).astype(F32)
        column = jnp.floor((lane + 0.5) * (1.0 / CAP))
        ahead = place - (column * height + (lane - column * CAP))
        group = [(n, zi, zat(offset)) for n, (at, zi, offset) in enumerate(sources) if at == buffer]
        spread = []
        for n, zi, where in group:
            weight = ag_m[where]
            for rel in (0, 1):
                table = (ahead == zi * PAIR + rel * CAP).astype(F32).astype(BF16)
                spread.append(dot(weight[rel * TM : (rel + 1) * TM], table))
        spread = jnp.concatenate(spread, axis=0).astype(BF16)
        for n in range(5):
            if PARCELS[n][0] == buffer:
                for r in range(1, NE):
                    ret_copy(n, r, columns[r]).wait_recv()

        def gather(cols):
            rows = ret_r[buffer][:, :, cols].reshape(NE * height, D // 4)
            result = dot(spread, rows)
            for at, (n, zi, where) in enumerate(group):
                acc[where, :, cols] += result[2 * at * TM : (2 * at + 1) * TM]
                oth[where, :, cols] = result[(2 * at + 1) * TM : (2 * at + 2) * TM].astype(BF16)

        wide(4, gather)
        for n, zi, where in group:
            oth_copy(n).start()

    mix_copy.wait_recv()
    mix_step(0)
    opposite = zat(4)
    for k in (0, 1):
        ag_wait(k, 3, CR0 + k)
        far_hid[k, pl.ds(2 * HALF, HALF)] = hidden(ag_r[opposite, k], wr)
        give_back(4, k * HB, HB, dot(far2_ref[...], far_hid[k]).astype(BF16))
    shared(zat(-3), zat(3))
    mix_step(1)
    ag_wait(0, 3, CO)
    ag_wait(1, 3, CM)
    shared(opposite)
    combine(0)
    mix_step(2)
    combine(1)
    mix_step(3)
    combine(2)
    for n in range(NZ):
        oth_copy(n).wait_recv()
    moe_step(0)
    mix_finish(mixer_ref)
    for s in (1, 2, 3):
        moe_step(s)
    moe_finish(channel_ref)

    for copy in pair + sent + [mix_copy]:
        copy.wait_send()
    for r in range(1, NE):
        a2a_copy(r, r).wait_send()
    each_later(lambda j: st_copy(j, me).wait_send())
    for way in (0, 1):
        ag_copy(way, 0, CO, z, first=True).wait_send()
        for hop in range(3):
            for chunk in (CO, CM, CR0, CR1):
                if hop or chunk != CO:
                    ag_copy(way, hop, chunk, z).wait_send()
    for way, chunk in ((0, CO), (1, CM), (0, CR0), (1, CR1)):
        ag_copy(way, 3, chunk, z).wait_send()
    for g in range(5):
        for r in range(1, NE):
            ret_copy(g, r, me).wait_send()
    for n in range(NZ):
        oth_copy(n).wait_send()
    mix_drain()
    moe_drain()


def fused(*args):
    vmem = pl.BlockSpec(memory_space=pltpu.VMEM)
    hbm = pl.BlockSpec(memory_space=pl.ANY)
    sem = pltpu.SemaphoreType.DMA
    scratch = [
        pltpu.VMEM((TM, D), BF16), pltpu.VMEM((1, D), F32), pltpu.VMEM((2, TM), jnp.int32),
        pltpu.VMEM((2, TM), F32), sem((4,)),
    ] + [
        pltpu.VMEM(s, t)
        for s, t in (
            ((1024, 128), BF16), ((1024, 128), BF16), ((1024, 256), BF16), ((1024, 256), BF16),
            ((NZ, BLOCK), F32), ((256, D), BF16),
            ((2, NE * PAD, 128), BF16), ((HALF, HB * PAD), BF16),
            ((HB * 16, 2 * HALF), BF16), ((HB * 32, 4 * HALF), BF16), ((HB * 16, 2 * HALF), BF16),
            ((HB * 16, 3 * HALF), BF16), ((4, 128, 128), F32),
            ((TM, D), BF16), ((4, TM, 128), BF16), ((1024, 128), BF16),
            ((2, D, 256), BF16), ((256, D), BF16), ((2, D, 256), BF16), ((256, D), BF16),
            ((TM, D), BF16), ((2, TM, 128), BF16),
            ((NE, PAD, D), BF16), ((NE, PAD, D), BF16),
            ((NZ, TM, D), BF16), ((NZ, 2 * TM, 128), BF16), ((NZ, 2, HALF, D), BF16),
            ((2, 4 * HALF, 256), BF16), ((2, 3 * HALF, 256), BF16),
            *(((NE, n, D), BF16) for n in HEIGHTS + HEIGHTS),
            ((NZ, TM, D), F32), ((NZ, TM, D), BF16), ((NZ, TM, D), BF16),
            ((2, NZ, 64, D), BF16), ((NZ, 64, D), BF16),
            ((2, 4, TM, D), BF16), ((2, 4, TM, D), BF16),
            ((2, 4, 64, D), BF16), ((2, 4, 64, D), BF16),
            ((144, 256), BF16), ((NE, 144, 256), BF16),
            ((NZ, BLOCK, 256), F32), ((BLOCK, 256), F32), ((BLOCK, 256), F32),
            ((NZ, BLOCK), F32), ((NZ, BLOCK), F32),
        )
    ] + [
        sem((13,)), sem((6,)), sem((6,)), sem((6,)), sem((3,)), sem((3,)), sem((NE,)), sem((NE,)),
        sem((2, 4, 4)), sem((2, 4, 4)), sem((NE,)), sem((NE,)),
        sem((5, NE)), sem((5, NE)), sem((NZ,)), sem((NZ,)), sem, sem,
        sem((2, 4, 4)), sem((2, 4, 4)), sem((2, 4, 4)), sem((2, 4, 4)),
    ]
    return pl.pallas_call(
        kernel,
        out_shape=(pltpu.VMEM((64, D), BF16), pltpu.VMEM((TM, D), BF16)),
        in_specs=[hbm] * 23,
        out_specs=(vmem, vmem),
        scratch_shapes=scratch,
        compiler_params=pltpu.CompilerParams(
            collective_id=0, has_side_effects=True, vmem_limit_bytes=60000000
        ),
    )(*args)


def local(
    query_rows, key_rows, value_rows, gate_rows, log_decay, out_weight, channel_input, norm_gain,
    routes, route_weight, expert_gate, expert_up, expert_down, shared_gate, shared_up, shared_down,
):
    return fused(
        channel_input, norm_gain.reshape(1, D), routes.T, route_weight.T,
        query_rows, key_rows, value_rows, gate_rows, log_decay.reshape(NZ, BLOCK), out_weight,
        expert_gate, expert_up, expert_down, shared_gate, shared_up, shared_down,
        *constants(),
    )


def solution(mesh):
    split = Mesh(mesh.devices.reshape(4, 4, NZ, 2), ALL)
    return jax.shard_map(
        local,
        mesh=split,
        in_specs=(
            P(EP, TP), P(EP, TP), P(EP, TP), P(EP, TP), P(TP, EP), P(TP, None),
            P(ALL, None), P(), P(ALL, None), P(ALL, None),
            P(EP, None, TP), P(EP, None, TP), P(EP, TP, None),
            P(None, TP), P(None, TP), P(TP, None),
        ),
        out_specs=(P(ALL, None), P(ALL, None)),
        check_vma=False,
    )
```

```python
import functools

import jax
import jax.numpy as jnp
import numpy as np
from jax import lax
from jax.experimental import pallas as pl
from jax.experimental.pallas import tpu as pltpu
from jax.sharding import Mesh
from jax.sharding import PartitionSpec as P

EP = ("y", "x")
TP = ("z", "c")
ALL = ("y", "x", "z", "c")
MESH = pl.DeviceIdType.MESH
F32 = jnp.float32
BF16 = jnp.bfloat16
epsilon = 1e-06
turn_base = 10000.0

D = 2048
NE = 16
NZ = 8
BLOCK = 128
CAP = 5
TM = 48
PAIR = 2 * CAP
ROWS = NE * PAIR
HALF = ROWS // 2
PAD = 16
CO, CM, CR0, CR1 = 0, 1, 2, 3
PARCELS = ((0, 0, 16), (1, 0, 16), (1, 16, 24), (2, 0, 16), (2, 16, 16))
HEIGHTS = (16, 48, 32)
BLOCKS = (
    (0, 0), (2, 2), (1, 3), (3, 1), (3, 3), (1, 1), (0, 2), (2, 0),
    (2, 3), (2, 1), (3, 2), (1, 2), (0, 3), (0, 1), (3, 0), (1, 0),
)
BACK = tuple(BLOCKS.index((-dy % 4, -dx % 4)) for dy, dx in BLOCKS)
HB = NE // 2


def dot(a, b, dims=None, precision=None):
    if dims is None:
        return jnp.dot(a, b, preferred_element_type=F32, precision=precision)
    return lax.dot_general(a, b, (dims, ((), ())), preferred_element_type=F32)


def silu(v):
    return v / (1.0 + jnp.exp(-v))


def constants():
    place = np.zeros((2, NE * PAD, 128), np.float32)
    select = np.zeros((HALF, HB * PAD), np.float32)
    near_first = np.zeros((HB * 16, 2 * HALF), np.float32)
    near_rest = np.zeros((HB * 32, 4 * HALF), np.float32)
    far_first = np.zeros((HB * 16, 2 * HALF), np.float32)
    far_rest = np.zeros((HB * 16, 3 * HALF), np.float32)
    for j in range(NE):
        for rel in range(2):
            for p in range(CAP):
                place[rel, j * PAD + rel * CAP + p, j * CAP + p] = 1
    for b in range(HB):
        for r in range(PAIR):
            select[b * PAIR + r, b * PAD + r] = 1
            for zi in range(4):
                row, column = zi * PAIR + r, zi * HALF + b * PAIR + r
                if row < 16:
                    near_first[b * 16 + row, column] = far_first[b * 16 + row, column] = 1
                else:
                    near_rest[b * 32 + row - 16, column] = 1
                    if zi < 3:
                        far_rest[b * 16 + row - 16, column] = 1
    rate = turn_base ** (-(np.arange(128) % 64) / 64.0)
    near = np.arange(BLOCK)[:, None] * rate
    far = np.arange(128)[:, None] * float(BLOCK) * rate
    turns = np.stack([np.cos(near), np.sin(near), np.cos(far), np.sin(far)])
    tables = (place, select, near_first, near_rest, far_first, far_rest)
    return [jnp.asarray(m, BF16) for m in tables] + [jnp.asarray(turns, F32)]


def kernel(
    chan_hbm, gain_hbm, routes_hbm, share_hbm,
    q_hbm, k_hbm, v_hbm, g_hbm, decay_hbm, ow_hbm,
    eg_ref, eu_ref, ed_ref, sg_ref, su_ref, sd_ref,
    cplace_hbm, cselect_hbm, near1_hbm, near2_hbm, far1_hbm, far2_hbm, turns_hbm,
    mixer_ref, channel_ref,
    chan_ref, gain_ref, routes_ref, share_ref, first_sem,
    q_ref, k_ref, v_ref, g_ref, decay_ref, ow_ref,
    cplace_ref, cselect_ref, near1_ref, near2_ref, far1_ref, far2_ref, turns_ref, normed_ref, meta_ref, keys,
    wr, wd, ws, wsd, pn, pm, outg, a2a, ag_o, ag_m, ag_r, near_hid, far_hid,
    ret0_s, ret1_s, ret2_s, ret0_r, ret1_r, ret2_r,
    acc, oth, othp, mix, mixp, rs_s, rs_r, rm_s, rm_r,
    st_s, st_r, before, state, entry, run_s, off_s,
    in_sem, load_sem, w_s, w_r, pair_s, pair_r, a2a_s, a2a_r, ag_s, ag_v, st_ss, st_rs,
    ret_ss, ret_rs, oth_s, oth_r, mixp_s, mixp_r, rs_ss, rs_rs, rm_ss, rm_rs,
):
    y, x, z, c = (lax.axis_index(a) for a in ALL)
    me = y * 4 + x
    pc = 1 - c
    zup, zdown = lax.rem(z + 1, NZ), lax.rem(z + NZ - 1, NZ)
    partner = {"c": pc}

    def zat(offset):
        return lax.rem(z + (offset + NZ), NZ)

    def peer(j):
        return {"y": lax.div(j, 4), "x": lax.rem(j, 4)}

    columns = [lax.rem(y + dy, 4) * 4 + lax.rem(x + dx, 4) for dy, dx in BLOCKS]

    def rcopy(src, dst, ss, rs, dev):
        return pltpu.make_async_remote_copy(
            src_ref=src, dst_ref=dst, send_sem=ss, recv_sem=rs, device_id=dev, device_id_type=MESH
        )

    firsts = [
        (chan_hbm, chan_ref), (gain_hbm, gain_ref), (routes_hbm, routes_ref), (share_hbm, share_ref),
    ]
    firsts = [pltpu.make_async_copy(s, d, first_sem.at[n]) for n, (s, d) in enumerate(firsts)]
    for copy in firsts:
        copy.start()
    ret_s, ret_r = (ret0_s, ret1_s, ret2_s), (ret0_r, ret1_r, ret2_r)
    ret1_r[:, pl.ds(32, 16), :] = jnp.zeros((NE, 16, D), BF16)
    barrier = pltpu.get_barrier_semaphore()
    for j in columns[1:]:
        pl.semaphore_signal(barrier, inc=1, device_id=peer(j), device_id_type=MESH)
    for dev in ({"z": zup}, {"z": zdown}, partner):
        pl.semaphore_signal(barrier, inc=1, device_id=dev, device_id_type=MESH)
    incoming = [
        (cplace_hbm, cplace_ref), (k_hbm, k_ref), (v_hbm, v_ref), (decay_hbm, decay_ref),
        (turns_hbm, turns_ref), (cselect_hbm, cselect_ref), (q_hbm, q_ref), (g_hbm, g_ref),
        (ow_hbm, ow_ref), (near1_hbm, near1_ref), (near2_hbm, near2_ref), (far1_hbm, far1_ref),
        (far2_hbm, far2_ref),
    ]
    arriving = [pltpu.make_async_copy(s, d, in_sem.at[n]) for n, (s, d) in enumerate(incoming)]
    for copy in arriving:
        copy.start()

    for copy in firsts:
        copy.wait()
    wide_rows = chan_ref[...].astype(F32)
    mean = jnp.mean(wide_rows * wide_rows, axis=-1, keepdims=True)
    normed_ref[...] = (wide_rows * lax.rsqrt(mean + epsilon) * gain_ref[...]).astype(BF16)
    lanes = lax.broadcasted_iota(jnp.int32, (TM, 128), 1).astype(F32)
    token_r = lax.broadcasted_iota(jnp.int32, (TM, TM), 0)
    token_c = lax.broadcasted_iota(jnp.int32, (TM, TM), 1)
    unit = (token_r == token_c).astype(F32)

    def upright(rows):
        flipped = lax.dot_general(
            unit, rows, (((1,), (1,)), ((), ())), precision=lax.Precision.HIGHEST,
            preferred_element_type=F32,
        )
        return [flipped[:, k : k + 1] for k in (0, 1)]

    picks = upright(routes_ref[...].astype(F32))
    gains = upright(share_ref[...])
    hits = [(lanes == pick).astype(F32) for pick in picks]
    strict = token_r > token_c
    earlier = dot(strict.astype(F32).astype(BF16), (hits[0] + hits[1]).astype(BF16))
    metas = [jnp.zeros((TM, 128), F32)] * 4
    for k in (0, 1):
        rank = jnp.sum(earlier * hits[k], axis=-1, keepdims=True)
        column = jnp.floor(picks[k] * 0.5)
        there = (lanes == column * CAP + rank).astype(F32)
        for parity in (0, 1):
            mine = there * (picks[k] - 2 * column == parity).astype(F32)
            metas[parity] += mine
            metas[2 + parity] += mine * gains[k]
    for n in range(4):
        meta_ref[n] = metas[n].astype(BF16)
    pl.semaphore_wait(barrier, NE + 2)

    pair = [
        rcopy(normed_ref, pn, pair_s.at[0], pair_r.at[0], partner),
        rcopy(meta_ref.at[pc], pm.at[0], pair_s.at[1], pair_r.at[1], partner),
        rcopy(meta_ref.at[2 + pc], pm.at[1], pair_s.at[2], pair_r.at[2], partner),
    ]
    for copy in pair:
        copy.start()

    def ag_copy(way, hop, chunk, src_z, first=False):
        buf = {CO: ag_o.at[src_z], CM: ag_m.at[src_z]}.get(chunk)
        if buf is None:
            buf = ag_r.at[src_z, chunk - CR0]
        src = normed_ref if first and chunk == CO else buf
        dev = {"z": zup if way == 0 else zdown}
        return rcopy(src, buf, ag_s.at[way, hop, chunk], ag_v.at[way, hop, chunk], dev)

    def ag_start(way, hop, chunk):
        ag_copy(way, hop, chunk, zat(-hop if way == 0 else hop)).start()

    def ag_wait(way, hop, chunk):
        ag_copy(way, hop, chunk, zat(-(hop + 1) if way == 0 else hop + 1)).wait_recv()

    for way in (0, 1):
        ag_copy(way, 0, CO, z, first=True).start()
    weights = [
        (eg_ref.at[pc], wr.at[1, :, pl.ds(0, 128)]),
        (eu_ref.at[pc], wr.at[1, :, pl.ds(128, 128)]),
        (ed_ref.at[pc], wd.at[pl.ds(128, 128)]),
        (sg_ref, ws.at[1, :, pl.ds(0, 128)]),
        (su_ref, ws.at[1, :, pl.ds(128, 128)]),
        (sd_ref, wsd.at[pl.ds(128, 128)]),
    ]
    sent = [rcopy(s, d, w_s.at[n], w_r.at[n], partner) for n, (s, d) in enumerate(weights)]
    loads = [
        (eg_ref.at[c], wr.at[0, :, pl.ds(0, 128)]),
        (eu_ref.at[c], wr.at[0, :, pl.ds(128, 128)]),
        (ed_ref.at[c], wd.at[pl.ds(0, 128)]),
        (sg_ref, ws.at[0, :, pl.ds(0, 128)]),
        (su_ref, ws.at[0, :, pl.ds(128, 128)]),
        (sd_ref, wsd.at[pl.ds(0, 128)]),
    ]
    loaded = [pltpu.make_async_copy(s, d, load_sem.at[n]) for n, (s, d) in enumerate(loads)]
    for copy in loaded:
        copy.start()
    ag_o[z] = normed_ref[...]
    ag_m[z, pl.ds(0, TM)] = meta_ref[2 + c]
    for copy in pair:
        copy.wait_recv()
    ag_m[z, pl.ds(TM, TM)] = pm[1]
    for way in (0, 1):
        ag_start(way, 0, CM)

    def wide(count, body):
        def step(n, carry):
            body(pl.ds(pl.multiple_of(n * (D // count), D // count), D // count))
            return carry

        lax.fori_loop(0, count, step, 0)

    arriving[0].wait()
    own_pick = dot(cplace_ref[0], meta_ref[c], ((1,), (1,))).astype(BF16)
    other_pick = dot(cplace_ref[1], pm[0], ((1,), (1,))).astype(BF16)

    def gather_rows(cols):
        rows = dot(own_pick, normed_ref[:, cols]) + dot(other_pick, pn[:, cols])
        outg[:, :, cols] = rows.astype(BF16).reshape(NE, PAD, D // 4)

    wide(4, gather_rows)

    def a2a_copy(r, slot):
        return rcopy(
            outg.at[columns[r]], a2a.at[slot], a2a_s.at[r], a2a_r.at[slot], peer(columns[r])
        )

    for r in range(1, NE):
        a2a_copy(r, BACK[r]).start()
    a2a[0] = outg[me]

    def relay_own(hop):
        for chunk in (CO, CM):
            for way in (0, 1):
                ag_wait(way, hop, chunk)
        if hop < 2:
            for chunk in (CO, CM):
                for way in (0, 1):
                    ag_start(way, hop + 1, chunk)
        else:
            ag_start(0, 3, CO)
            ag_start(1, 3, CM)

    for copy in arriving[1:5]:
        copy.wait()
    half_lane = lax.broadcasted_iota(jnp.int32, (BLOCK, BLOCK), 1) < 64

    def turned(ref, n):
        rows = ref[pl.ds(pl.multiple_of(n * BLOCK, BLOCK), BLOCK), :].astype(F32)
        far_line = pl.ds(me * NZ + n, 1)
        near_cos, near_sin = turns_ref[0], turns_ref[1]
        far_cos, far_sin = turns_ref[2, far_line, :], turns_ref[3, far_line, :]
        cosine = far_cos * near_cos - far_sin * near_sin
        sine = far_sin * near_cos + far_cos * near_sin
        swapped = pltpu.roll(rows, 64, 1)
        return (rows * cosine + swapped * jnp.where(half_lane, -sine, sine)).astype(BF16)

    rows_i = lax.broadcasted_iota(jnp.int32, (BLOCK, BLOCK), 0)
    cols_i = lax.broadcasted_iota(jnp.int32, (BLOCK, BLOCK), 1)
    upper = (rows_i <= cols_i).astype(F32)
    lower = rows_i >= cols_i
    run_s[...] = dot(decay_ref[...], upper, precision=lax.Precision.HIGHEST)
    state[...] = jnp.zeros_like(state)

    def along(row):
        return jnp.transpose(jnp.broadcast_to(row, (BLOCK, BLOCK)))

    def local_state(n, total):
        rows = pl.ds(pl.multiple_of(n * BLOCK, BLOCK), BLOCK)
        row = run_s[pl.ds(n, 1), :]
        end = row[:, BLOCK - 1 :]
        off_s[pl.ds(n, 1), :] = jnp.broadcast_to(total, (1, BLOCK))
        tail = jnp.exp(end - along(row))
        key = turned(k_ref, n)
        keys[rows, :] = key
        keyed = (key.astype(F32) * tail).astype(BF16)
        before[n] = state[...]
        state[...] = jnp.exp(end) * state[...] + dot(keyed, v_ref[rows, :], ((0,), (0,)))
        return total + end

    total = lax.fori_loop(0, NZ, local_state, jnp.zeros((1, 1), F32))
    st_s[pl.ds(0, BLOCK), :] = state[...].astype(BF16)
    high = total.astype(BF16).astype(F32)
    middle = (total - high).astype(BF16).astype(F32)
    low = total - high - middle
    line = lax.broadcasted_iota(jnp.int32, (16, 256), 0)
    pieces = jnp.where(line == 0, high, jnp.where(line == 1, middle, jnp.where(line == 2, low, 0.0)))
    st_s[pl.ds(BLOCK, 16), :] = pieces.astype(BF16)

    def st_copy(j, slot):
        return rcopy(st_s, st_r.at[slot], st_ss.at[j], st_rs.at[slot], peer(j))

    def each_later(body):
        for j in columns[1:]:

            @pl.when(j > me)
            def _():
                body(j)

    relay_own(0)
    for copy in sent:
        copy.start()

    arriving[5].wait()
    for k in (0, 1):
        for r in range(max(1, k * HB), (k + 1) * HB):
            a2a_copy(r, r).wait_recv()
        if k == 0:
            each_later(lambda j: st_copy(j, me).start())

        def pack_rows(cols):
            rows = dot(cselect_ref[...], a2a[pl.ds(k * HB, HB), :, cols].reshape(HB * PAD, D // 4))
            ag_r[z, k, :, cols] = rows.astype(BF16)

        wide(4, pack_rows)
        for way in (0, 1):
            ag_start(way, 0, CR0 + k)
        if k == 0:
            relay_own(1)
    for copy in loaded + arriving[9:]:
        copy.wait()
    for copy in sent:
        copy.wait_recv()

    def hidden(rows, weight):
        parts = []
        for n in (0, 1):
            both = dot(rows, weight[n])
            parts.append((silu(both[:, :128]) * both[:, 128:]).astype(BF16))
        return jnp.concatenate(parts, axis=1)

    def shared(za, zb=None):
        rows = ag_o[za] if zb is None else jnp.concatenate([ag_o[za], ag_o[zb]], axis=0)
        h = hidden(rows, ws)

        def down(cols):
            result = dot(h, wsd[:, cols])
            acc[za, :, cols] = result[:TM]
            if zb is not None:
                acc[zb, :, cols] = result[TM:]

        wide(4, down)

    def ret_copy(n, r, slot):
        buffer, first, count = PARCELS[n]
        rows = pl.ds(first, count)
        return rcopy(
            ret_s[buffer].at[r, rows], ret_r[buffer].at[slot, rows], ret_ss.at[n, r],
            ret_rs.at[n, slot], peer(columns[r]),
        )

    def give_back(n, first, count, placed):
        buffer, top, _ = PARCELS[n]
        height = placed.shape[0] // count

        def down(cols):
            result = dot(placed, wd[:, cols]).astype(BF16)
            ret_s[buffer][pl.ds(first, count), pl.ds(top, height), cols] = result.reshape(
                count, height, D // 4
            )

        wide(4, down)
        for r in range(max(first, 1), first + count):
            ret_copy(n, r, me).start()
        if first == 0:
            rows = pl.ds(top, height)
            ret_r[buffer][me, rows] = ret_s[buffer][0, rows]

    own_hidden = hidden(ag_r[z].reshape(ROWS, D), wr)
    own_placed = [
        dot(cselect_ref[...], own_hidden[k * HALF : (k + 1) * HALF], ((0,), (0,))).astype(BF16)
        for k in (0, 1)
    ]
    give_back(0, 0, NE, jnp.concatenate(own_placed, axis=0))
    shared(z)

    entry[...] = jnp.zeros_like(entry)

    def take_state(j, carry):
        @pl.when(j < me)
        def _():
            st_copy(j, j).wait_recv()
            sums = st_r[j, pl.ds(BLOCK, 16), :].astype(F32)
            decay = jnp.exp(sums[0:1] + sums[1:2] + sums[2:3])
            entry[...] = decay * entry[...] + st_r[j, pl.ds(0, BLOCK), :].astype(F32)

        return carry


    def retain(n, carry):
        rows = pl.ds(pl.multiple_of(n * BLOCK, BLOCK), BLOCK)
        row = run_s[pl.ds(n, 1), :]
        spread = along(row)
        query, key, value = turned(q_ref, n), keys[rows, :], v_ref[rows, :]
        scores = dot(query, key, ((1,), (1,)))
        factor = jnp.exp(jnp.where(lower, spread - row, 0.0))
        mixed = jnp.where(lower, scores * factor, 0.0).astype(BF16)
        scaled_query = (query.astype(F32) * jnp.exp(spread)).astype(BF16)
        offset = jnp.exp(off_s[pl.ds(n, 1), :][:, 0:1])
        prior = (before[n] + offset * entry[...]).astype(BF16)
        kept = dot(mixed, value) + dot(scaled_query, prior)
        scale = lax.rsqrt(jnp.mean(kept * kept, axis=-1, keepdims=True) + epsilon)
        gated = (silu(g_ref[rows, :].astype(F32)) * (kept * scale)).astype(BF16)

        def project(cols):
            term = dot(gated, ow_ref[:, cols]).astype(BF16)
            mix[0, n, :, cols] = term[:64]
            mix[1, n, :, cols] = term[64:]

        wide(4, project)
        return carry

    mix_copy = rcopy(mix.at[pc], mixp, mixp_s, mixp_r, partner)

    def retain_some(first, last):
        lax.fori_loop(first, last, retain, 0)

    for h in (1, 2, 3):
        za, zb = zat(-h), zat(h)
        for k in (0, 1):
            for way in (0, 1):
                ag_wait(way, h - 1, CR0 + k)
            for way in (0, 1):
                if h < 3 or way == k:
                    ag_start(way, h, CR0 + k)
            h_rows = hidden(jnp.concatenate([ag_r[za, k], ag_r[zb, k]], axis=0), wr)
            if h == 1:
                near_hid[k, pl.ds(0, 2 * HALF)] = h_rows
                give_back(1, k * HB, HB, dot(near1_ref[...], h_rows).astype(BF16))
            elif h == 2:
                near_hid[k, pl.ds(2 * HALF, 2 * HALF)] = h_rows
                give_back(2, k * HB, HB, dot(near2_ref[...], near_hid[k]).astype(BF16))
            else:
                far_hid[k, pl.ds(0, 2 * HALF)] = h_rows
                give_back(3, k * HB, HB, dot(far1_ref[...], h_rows).astype(BF16))
            if (h, k) == (1, 0):
                relay_own(2)
                shared(za, zb)
            elif (h, k) == (1, 1):
                for copy in arriving[6:9]:
                    copy.wait()
                lax.fori_loop(0, NE - 1, take_state, 0)
                retain_some(0, 1)
            elif (h, k) == (2, 0):
                retain_some(1, 5)
            elif (h, k) == (2, 1):
                shared(za, zb)
            elif (h, k) == (3, 0):
                retain_some(5, 8)
                mix_copy.start()

    def chain(base, send, recv, ss, rs):
        width = D // 4

        def copy(way, s, part):
            dev = {"z": zup if way == 0 else zdown}
            cols = pl.ds(part * width, width)
            return rcopy(
                send.at[way, s, :, cols], recv.at[way, s, :, cols], ss.at[way, s, part],
                rs.at[way, s, part], dev,
            )

        def forward(s, part):
            for way in (0, 1):
                hop = s if part // 2 == way else s + 1
                if hop > 3:
                    continue
                target = zat(4 - hop if way == 0 else hop - 4)
                cols = pl.ds(part * width, width)
                value = base(target, cols)
                if s > 0:
                    copy(way, hop - 1, part).wait_recv()
                    value = value + recv[way, hop - 1, :, cols].astype(F32)
                send[way, hop, :, cols] = value.astype(BF16)
                copy(way, hop, part).start()

        def step(s):
            for part in (0, 2, 1, 3):
                forward(s, part)

        def finish(out_ref):
            for part in (0, 2, 1, 3):
                cols = pl.ds(part * width, width)
                value = base(z, cols)
                for way in (0, 1):
                    copy(way, 3, part).wait_recv()
                    value = value + recv[way, 3, :, cols].astype(F32)
                out_ref[:, cols] = value.astype(BF16)

        def drain():
            for way in (0, 1):
                for s in range(4):
                    for part in range(4):
                        if s or part // 2 == way:
                            copy(way, s, part).wait_send()

        return step, finish, drain

    def mix_base(target, cols):
        return mix[c, target, :, cols].astype(F32) + mixp[target, :, cols].astype(F32)

    def moe_base(target, cols):
        return acc[target, :, cols] + othp[target, :, cols].astype(F32)

    mix_step, mix_finish, mix_drain = chain(mix_base, rm_s, rm_r, rm_ss, rm_rs)
    moe_step, moe_finish, moe_drain = chain(moe_base, rs_s, rs_r, rs_ss, rs_rs)

    sources = [(0, 0, 0), (1, 0, -1), (1, 1, 1), (1, 2, -2), (1, 3, 2), (2, 0, -3), (2, 1, 3), (2, 2, 4)]

    def oth_copy(n):
        where = zat(sources[n][2])
        return rcopy(oth.at[where], othp.at[where], oth_s.at[n], oth_r.at[n], partner)

    def combine(buffer):
        height = HEIGHTS[buffer]
        lane = lax.broadcasted_iota(jnp.int32, (128, NE * height), 0).astype(F32)
        place = lax.broadcasted_iota(jnp.int32, (128, NE * height), 1).astype(F32)
        column = jnp.floor((lane + 0.5) * (1.0 / CAP))
        ahead = place - (column * height + (lane - column * CAP))
        group = [(n, zi, zat(offset)) for n, (at, zi, offset) in enumerate(sources) if at == buffer]
        spread = []
        for n, zi, where in group:
            weight = ag_m[where]
            for rel in (0, 1):
                table = (ahead == zi * PAIR + rel * CAP).astype(F32).astype(BF16)
                spread.append(dot(weight[rel * TM : (rel + 1) * TM], table))
        spread = jnp.concatenate(spread, axis=0).astype(BF16)
        for n in range(5):
            if PARCELS[n][0] == buffer:
                for r in range(1, NE):
                    ret_copy(n, r, columns[r]).wait_recv()

        def gather(cols):
            rows = ret_r[buffer][:, :, cols].reshape(NE * height, D // 4)
            result = dot(spread, rows)
            for at, (n, zi, where) in enumerate(group):
                acc[where, :, cols] += result[2 * at * TM : (2 * at + 1) * TM]
                oth[where, :, cols] = result[(2 * at + 1) * TM : (2 * at + 2) * TM].astype(BF16)

        wide(4, gather)
        for n, zi, where in group:
            oth_copy(n).start()

    mix_copy.wait_recv()
    mix_step(0)
    opposite = zat(4)
    for k in (0, 1):
        ag_wait(k, 3, CR0 + k)
        far_hid[k, pl.ds(2 * HALF, HALF)] = hidden(ag_r[opposite, k], wr)
        give_back(4, k * HB, HB, dot(far2_ref[...], far_hid[k]).astype(BF16))
    shared(zat(-3), zat(3))
    mix_step(1)
    ag_wait(0, 3, CO)
    ag_wait(1, 3, CM)
    shared(opposite)
    combine(0)
    mix_step(2)
    combine(1)
    mix_step(3)
    combine(2)
    for n in range(NZ):
        oth_copy(n).wait_recv()
    moe_step(0)
    mix_finish(mixer_ref)
    for s in (1, 2, 3):
        moe_step(s)
    moe_finish(channel_ref)

    for copy in pair + sent + [mix_copy]:
        copy.wait_send()
    for r in range(1, NE):
        a2a_copy(r, r).wait_send()
    each_later(lambda j: st_copy(j, me).wait_send())
    for way in (0, 1):
        ag_copy(way, 0, CO, z, first=True).wait_send()
        for hop in range(3):
            for chunk in (CO, CM, CR0, CR1):
                if hop or chunk != CO:
                    ag_copy(way, hop, chunk, z).wait_send()
    for way, chunk in ((0, CO), (1, CM), (0, CR0), (1, CR1)):
        ag_copy(way, 3, chunk, z).wait_send()
    for g in range(5):
        for r in range(1, NE):
            ret_copy(g, r, me).wait_send()
    for n in range(NZ):
        oth_copy(n).wait_send()
    mix_drain()
    moe_drain()


def fused(*args):
    vmem = pl.BlockSpec(memory_space=pltpu.VMEM)
    hbm = pl.BlockSpec(memory_space=pl.ANY)
    sem = pltpu.SemaphoreType.DMA
    scratch = [
        pltpu.VMEM((TM, D), BF16), pltpu.VMEM((1, D), F32), pltpu.VMEM((2, TM), jnp.int32),
        pltpu.VMEM((2, TM), F32), sem((4,)),
    ] + [
        pltpu.VMEM(s, t)
        for s, t in (
            ((1024, 128), BF16), ((1024, 128), BF16), ((1024, 256), BF16), ((1024, 256), BF16),
            ((NZ, BLOCK), F32), ((256, D), BF16),
            ((2, NE * PAD, 128), BF16), ((HALF, HB * PAD), BF16),
            ((HB * 16, 2 * HALF), BF16), ((HB * 32, 4 * HALF), BF16), ((HB * 16, 2 * HALF), BF16),
            ((HB * 16, 3 * HALF), BF16), ((4, 128, 128), F32),
            ((TM, D), BF16), ((4, TM, 128), BF16), ((1024, 128), BF16),
            ((2, D, 256), BF16), ((256, D), BF16), ((2, D, 256), BF16), ((256, D), BF16),
            ((TM, D), BF16), ((2, TM, 128), BF16),
            ((NE, PAD, D), BF16), ((NE, PAD, D), BF16),
            ((NZ, TM, D), BF16), ((NZ, 2 * TM, 128), BF16), ((NZ, 2, HALF, D), BF16),
            ((2, 4 * HALF, 256), BF16), ((2, 3 * HALF, 256), BF16),
            *(((NE, n, D), BF16) for n in HEIGHTS + HEIGHTS),
            ((NZ, TM, D), F32), ((NZ, TM, D), BF16), ((NZ, TM, D), BF16),
            ((2, NZ, 64, D), BF16), ((NZ, 64, D), BF16),
            ((2, 4, TM, D), BF16), ((2, 4, TM, D), BF16),
            ((2, 4, 64, D), BF16), ((2, 4, 64, D), BF16),
            ((144, 256), BF16), ((NE, 144, 256), BF16),
            ((NZ, BLOCK, 256), F32), ((BLOCK, 256), F32), ((BLOCK, 256), F32),
            ((NZ, BLOCK), F32), ((NZ, BLOCK), F32),
        )
    ] + [
        sem((13,)), sem((6,)), sem((6,)), sem((6,)), sem((3,)), sem((3,)), sem((NE,)), sem((NE,)),
        sem((2, 4, 4)), sem((2, 4, 4)), sem((NE,)), sem((NE,)),
        sem((5, NE)), sem((5, NE)), sem((NZ,)), sem((NZ,)), sem, sem,
        sem((2, 4, 4)), sem((2, 4, 4)), sem((2, 4, 4)), sem((2, 4, 4)),
    ]
    return pl.pallas_call(
        kernel,
        out_shape=(pltpu.VMEM((64, D), BF16), pltpu.VMEM((TM, D), BF16)),
        in_specs=[hbm] * 23,
        out_specs=(vmem, vmem),
        scratch_shapes=scratch,
        compiler_params=pltpu.CompilerParams(
            collective_id=0, has_side_effects=True, vmem_limit_bytes=60000000
        ),
    )(*args)


def local(
    query_rows, key_rows, value_rows, gate_rows, log_decay, out_weight, channel_input, norm_gain,
    routes, route_weight, expert_gate, expert_up, expert_down, shared_gate, shared_up, shared_down,
):
    return fused(
        channel_input, norm_gain.reshape(1, D), routes.T, route_weight.T,
        query_rows, key_rows, value_rows, gate_rows, log_decay.reshape(NZ, BLOCK), out_weight,
        expert_gate, expert_up, expert_down, shared_gate, shared_up, shared_down,
        *constants(),
    )


def solution(mesh):
    split = Mesh(mesh.devices.reshape(4, 4, NZ, 2), ALL)
    return jax.shard_map(
        local,
        mesh=split,
        in_specs=(
            P(EP, TP), P(EP, TP), P(EP, TP), P(EP, TP), P(TP, EP), P(TP, None),
            P(ALL, None), P(), P(ALL, None), P(ALL, None),
            P(EP, None, TP), P(EP, None, TP), P(EP, TP, None),
            P(None, TP), P(None, TP), P(TP, None),
        ),
        out_specs=(P(ALL, None), P(ALL, None)),
        check_vma=False,
    )
```
